512 devices in a mesh: grp: 2 (over y), tp: 32 (over z), dp: 8 (over x, core).
Axes of the slice: x: 4, y: 2, z: 32, core: 2. Of those that a mesh axis runs over, the one named last changes fastest.
The devices are a block of a 4x8x32 slice.
Arguments:
- hidden_in: bfloat16 [192, 4096], P(('grp', 'tp'), 'dp'), parts along dimension 0, may hold values from -40 to 40
- input_norm_gain: float32 [2, 4096], P(None, 'dp'), may hold values from 0.1 to 1.9
- w_query: bfloat16 [2, 4096, 2048], P(None, 'dp', 'tp'), may hold values from -0.09375 to 0.09375
- w_key: bfloat16 [2, 4096, 2048], P(None, 'dp', 'tp'), may hold values from -0.09375 to 0.09375
- w_decay: bfloat16 [2, 4096, 2048], P(None, 'dp', 'tp'), may hold values from -0.375 to 0.375
- w_value: bfloat16 [2, 4096, 4096], P(None, 'dp', 'tp'), may hold values from -0.09375 to 0.09375
- w_gate: bfloat16 [2, 4096, 4096], P(None, 'dp', 'tp'), may hold values from -0.09375 to 0.09375
- out_gain: float32 [2, 4096], P(None, 'tp'), may hold values from 0.1 to 1.9
- w_out: bfloat16 [2, 4096, 4096], P(None, 'tp', 'dp'), may hold values from -0.09375 to 0.09375
- decay_offset: float32 [2, 192, 2048], P(None, ('grp', 'dp'), 'tp'), parts along dimension 1, may hold values from -0.7 to 0
- state: float32 [2, 192, 32, 64, 128], P(None, ('grp', 'dp'), 'tp'), parts along dimension 1, may hold values from -3 to 3
Outputs:
- hidden_out: bfloat16 [192, 4096], P(('grp', 'tp'), 'dp'), parts along dimension 0
- new_state: float32 [2, 192, 32, 64, 128], P(None, ('grp', 'dp'), 'tp'), parts along dimension 1
The draws below stay inside these ranges and needn't reach their ends.
There are 2 independent parts, one for each index of `grp`. The reference program is written for one: setup_inputs(seed, part) draws one part's arguments, and reference() takes and returns one part's arrays. A program takes and returns all parts, laid end to end along the dimension named above; an argument that names none is the same for every part. Nothing has to cross between parts.
All inputs are finite; a program needn't handle non-finite values.
Results may differ from the reference program's by a relative error of at most 0.017.
Values may be sent and summed in bfloat16 or wider, within the bound.
A program may use at most 64 MiB of HBM per device.

```python
import jax
import jax.numpy as jnp
from jax import lax

D = 4096
HEADS = 32
HEAD_KEY = 64
VALUE_CHANNELS = 128
LAYERS = 2
BATCH = 96
KEY_W = 2048
VAL_W = 4096
N_DP = 8


def draw_hidden_in(key, part):
    base_key, column_key, row_key = jax.random.split(key, 3)
    column = jnp.arange(D, dtype=jnp.float32) / (D - 1)
    column_scale = jnp.exp(jnp.log(3.0) * column + jax.random.uniform(column_key, (D,), jnp.float32, -0.5, 0.5))
    values = jnp.clip(jax.random.normal(base_key, (BATCH, D), jnp.float32), -4.0, 4.0)
    row_scale = jnp.exp(jax.random.uniform(row_key, (BATCH, 1), jnp.float32, -0.7, 0.7))
    return (values * row_scale * column_scale[None, :]).astype(jnp.bfloat16)


def level_of(own_key, extent, shards, low, largest):
    level = 1.0
    for position, blocks in shards:
        steps = jax.random.uniform(jax.random.fold_in(jax.random.fold_in(own_key, 6), position), (blocks,), jnp.float32, low / len(shards), largest / len(shards))
        level = level * jnp.repeat(jnp.exp(steps), extent[position] // blocks).reshape((-1,) + (1,) * (len(extent) - 1 - position))
    return level


def bell_draw(stream_key, dims, scale, bound, cuts=(), kind=jnp.bfloat16):
    result = scale * jax.random.normal(stream_key, dims, jnp.float32)
    if cuts:
        result = result * level_of(stream_key, dims, cuts, -0.22, 0.18)
    return jnp.clip(result, -bound, bound).astype(kind)


def setup_inputs(seed: int = 0, part: int = 0) -> dict:
    arg_keys = jax.random.split(jax.random.key(seed), 12)
    part_keys = jax.random.split(jax.random.fold_in(arg_keys[11], part), 12)
    hidden_in = draw_hidden_in(jax.random.fold_in(jax.random.fold_in(arg_keys[11], part), 71), part)
    input_norm_gain = jnp.clip(1.0 + 0.18 * jax.random.normal(arg_keys[1], (LAYERS, D), jnp.float32), 0.1, 1.9)
    w_query = bell_draw(arg_keys[2], (LAYERS, D, KEY_W), D ** -0.5, 0.09375, ((1, 8), (2, 32)))
    w_key = bell_draw(arg_keys[3], (LAYERS, D, KEY_W), D ** -0.5, 0.09375, ((1, 8), (2, 32)))
    w_decay = bell_draw(arg_keys[4], (LAYERS, D, KEY_W), (D // 16) ** -0.5, 0.375, ((1, 8), (2, 32)))
    w_value = bell_draw(arg_keys[5], (LAYERS, D, VAL_W), D ** -0.5, 0.09375, ((1, 8), (2, 32)))
    w_gate = bell_draw(arg_keys[6], (LAYERS, D, VAL_W), D ** -0.5, 0.09375, ((1, 8), (2, 32)))
    out_gain = jnp.clip(1.0 + 0.18 * jax.random.normal(arg_keys[7], (LAYERS, VAL_W), jnp.float32), 0.1, 1.9)
    w_out = bell_draw(arg_keys[8], (LAYERS, VAL_W, D), VAL_W ** -0.5, 0.09375, ((1, 32), (2, 8)))
    decay_offset = jnp.clip(-0.7 + 0.7 * jax.random.uniform(part_keys[9], (LAYERS, BATCH, KEY_W), jnp.float32) ** level_of(part_keys[9], (LAYERS, BATCH, KEY_W), ((1, 8), (2, 32)), -0.2, 0.2), -0.7, 0.0)
    state = bell_draw(part_keys[10], (LAYERS, BATCH, HEADS, HEAD_KEY, VALUE_CHANNELS), 0.5, 3.0, ((1, 8), (2, 32)), jnp.float32)
    return dict(hidden_in=hidden_in, input_norm_gain=input_norm_gain, w_query=w_query, w_key=w_key, w_decay=w_decay, w_value=w_value, w_gate=w_gate, out_gain=out_gain, w_out=w_out, decay_offset=decay_offset, state=state)


epsilon = 1e-06
softness_factor = 16.0

def reference(hidden_in, input_norm_gain, w_query, w_key, w_decay, w_value, w_gate, out_gain, w_out, decay_offset, state):
    hidden = hidden_in
    states = []
    for index_of_block in range(LAYERS):
        widened = hidden.astype(jnp.float32)
        squares = lax.optimization_barrier(jnp.sum(widened * widened, axis=1))
        scaled_query = (widened * input_norm_gain[index_of_block][None, :]).astype(jnp.bfloat16)
        groups = scaled_query.astype(jnp.float32).reshape(BATCH, N_DP, D // N_DP)
        pieces = []
        for matrix in (w_query, w_key, w_decay, w_value, w_gate):
            blocks = matrix[index_of_block].astype(jnp.float32).reshape(N_DP, D // N_DP, matrix.shape[2])
            partial_value = jnp.einsum('bnr,nrc->nbc', groups, blocks, precision=lax.Precision.HIGHEST)
            rounded = lax.optimization_barrier(partial_value.astype(jnp.bfloat16))
            pieces.append(lax.optimization_barrier(jnp.sum(rounded.astype(jnp.float32), axis=0)))
        inverse = lax.rsqrt(squares / D + epsilon)[:, None]
        query_rows = (pieces[0] * inverse).reshape(BATCH, HEADS, HEAD_KEY)
        key_rows = (pieces[1] * inverse).reshape(BATCH, HEADS, HEAD_KEY) * HEAD_KEY ** (-0.5)
        decay_logits = pieces[2] * inverse
        value_rows = (pieces[3] * inverse).reshape(BATCH, HEADS, VALUE_CHANNELS)
        gate_rows = (pieces[4] * inverse).reshape(BATCH, HEADS, VALUE_CHANNELS)
        decay_logarithm = jax.nn.log_sigmoid(decay_logits) / softness_factor + decay_offset[index_of_block]
        decay_rate = jnp.exp(decay_logarithm).reshape(BATCH, HEADS, HEAD_KEY)
        fresh = decay_rate[:, :, :, None] * state[index_of_block] + key_rows[:, :, :, None] * value_rows[:, :, None, :]
        readout = lax.optimization_barrier(jnp.sum(query_rows[:, :, :, None] * fresh, axis=2))
        normed = readout * lax.rsqrt(lax.optimization_barrier(jnp.mean(readout * readout, axis=2, keepdims=True)) + epsilon)
        normed = normed * out_gain[index_of_block].reshape(HEADS, VALUE_CHANNELS)[None]
        gated_out = (normed * jax.nn.silu(gate_rows)).reshape(BATCH, VAL_W).astype(jnp.bfloat16)
        mixed = jnp.dot(gated_out, w_out[index_of_block], preferred_element_type=jnp.float32)
        hidden = (widened + mixed).astype(jnp.bfloat16)
        states.append(fresh)
    return (hidden, jnp.stack(states))
```

```python
import functools

import jax
import jax.numpy as jnp
from jax import lax
from jax.experimental import pallas as pl
from jax.experimental.pallas import tpu as pltpu
from jax.sharding import PartitionSpec as P

D = 4096
HEAD_KEY = 64
VALUE_CHANNELS = 128
LAYERS = 2

epsilon = 1e-06
softness_factor = 16.0

MESH = pl.DeviceIdType.MESH


def kernel(
    n_tp,
    n_dp,
    hidden,
    gain,
    w_query,
    w_key,
    w_decay,
    w_value,
    w_gate,
    out_gain,
    w_out,
    decay_offset,
    state,
    hidden_out,
    new_state,
    h_v,
    gain_v,
    qkd_v,
    wcat,
    ogain_v,
    wout_v,
    off_v,
    st,
    ag,
    part_send,
    part_recv,
    gat,
    rs_send,
    rs_recv,
    xs,
    pk,
    local_sem,
    state_sem,
    out_sem,
    ag_send_sem,
    ag_sem,
    part_send_sem,
    part_sem,
    gat_send_sem,
    gat_sem,
    rs_send_sem,
    rs_sem,
):
    rows, feats = h_v.shape
    half = feats // 2
    members = n_tp // n_dp
    seqs = rows * members
    p = lax.axis_index("tp")
    d = lax.axis_index("dp")
    group = p // members
    place = p % members
    anti = (p + n_tp // 2) % n_tp
    near_first = jnp.where(2 * place >= members, 1, -1)

    barrier = pltpu.get_barrier_semaphore()

    def greet_tp(i, c):
        pl.semaphore_signal(
            barrier, inc=1, device_id={"tp": (p + 1 + i) % n_tp}, device_id_type=MESH
        )
        return c

    def greet_dp(i, c):
        pl.semaphore_signal(
            barrier, inc=1, device_id={"dp": (d + 1 + i) % n_dp}, device_id_type=MESH
        )
        return c

    lax.fori_loop(0, n_tp - 1, greet_tp, 0)
    lax.fori_loop(0, n_dp - 1, greet_dp, 0)

    fetches = [
        pltpu.make_async_copy(hidden, h_v, local_sem.at[0]),
        pltpu.make_async_copy(gain, gain_v, local_sem.at[1]),
        pltpu.make_async_copy(w_query, qkd_v.at[0], local_sem.at[2]),
        pltpu.make_async_copy(w_key, qkd_v.at[1], local_sem.at[3]),
        pltpu.make_async_copy(w_decay, qkd_v.at[2], local_sem.at[4]),
        pltpu.make_async_copy(w_value, wcat.at[:, :, pl.ds(256, 128)], local_sem.at[5]),
        pltpu.make_async_copy(w_gate, wcat.at[:, :, pl.ds(384, 128)], local_sem.at[6]),
        pltpu.make_async_copy(out_gain, ogain_v, local_sem.at[7]),
        pltpu.make_async_copy(w_out, wout_v, local_sem.at[8]),
        pltpu.make_async_copy(decay_offset, off_v, local_sem.at[9]),
    ]
    for f in fetches:
        f.start()
    state_in = [
        pltpu.make_async_copy(state.at[l, :, 0], st.at[l], state_sem.at[l]) for l in range(LAYERS)
    ]
    for f in state_in:
        f.start()
    for f in fetches:
        f.wait()

    xs[...] = jnp.zeros_like(xs)

    first = h_v[...].astype(jnp.float32)
    pk[0, 0:1, 0:feats] = first[0:1]
    pk[0, 0:1, feats : feats + half] = first[1:2, 0:half]
    pk[0, 1:2, 0:half] = first[1:2, half:feats]
    pk[0, 1:2, half : half + feats] = first[2:3]
    ag[0, p] = pk[0].astype(jnp.bfloat16)

    for l in range(LAYERS):
        wcat[l, :, 0:128] = jnp.concatenate([qkd_v[0, l], qkd_v[1, l]], axis=-1)
        wcat[l, :, 128:256] = jnp.concatenate(
            [qkd_v[2, l], jnp.zeros_like(qkd_v[2, l])], axis=-1
        )

    pl.semaphore_wait(barrier, n_tp - 1 + n_dp - 1)

    def source_group(i):
        k = (i + 1) // 2
        side = jnp.where(i % 2 == 1, near_first, -near_first)
        return (group + n_dp + side * k) % n_dp

    def row_group(l, i):
        return (source_group(i) + l * (n_dp // 2)) % n_dp

    def gather_copy(l, peer):
        return pltpu.make_async_remote_copy(
            src_ref=ag.at[l, p],
            dst_ref=ag.at[l, p],
            send_sem=ag_send_sem.at[l],
            recv_sem=ag_sem.at[l, group],
            device_id={"tp": peer},
            device_id_type=MESH,
        )

    def gather_start(l):
        def one(i, c):
            k = n_tp // 2 - (i + 1) // 2
            off = jnp.where(i % 2 == 1, k, n_tp - k)
            gather_copy(l, (p + off) % n_tp).start()
            return c

        lax.fori_loop(0, n_tp - 1, one, 0)

    def gather_wait(l, sg, first_slot, count):
        block = ag.at[l, pl.ds(first_slot, count)]
        pltpu.make_async_remote_copy(
            src_ref=block,
            dst_ref=block,
            send_sem=ag_send_sem.at[l],
            recv_sem=ag_sem.at[l, sg],
            device_id={"tp": anti},
            device_id_type=MESH,
        ).wait_recv()

    def part_copy(l, i, to):
        slot = (d - to + n_dp) % n_dp - 1
        return pltpu.make_async_remote_copy(
            src_ref=part_send.at[l, i],
            dst_ref=part_recv.at[l, slot],
            send_sem=part_send_sem.at[l],
            recv_sem=part_sem.at[l],
            device_id={"dp": to},
            device_id_type=MESH,
        )

    lane = lax.broadcasted_iota(jnp.int32, (seqs, 512), 1)

    def project(l, i):
        sg = source_group(i)
        for j in range(members):
            b = ag[l, sg * members + j].astype(jnp.float32)
            xs[3 * j : 3 * j + 1, :] = b[0:1, 0:feats]
            xs[3 * j + 1 : 3 * j + 2, 0:half] = b[0:1, feats : feats + half]
            xs[3 * j + 1 : 3 * j + 2, half:feats] = b[1:2, 0:half]
            xs[3 * j + 2 : 3 * j + 3, :] = b[1:2, half : half + feats]
        x = xs[...]
        squares = jnp.sum(x * x, axis=1, keepdims=True)[0:seqs]
        scaled = (x * gain_v[l : l + 1, :]).astype(jnp.bfloat16)
        y = jnp.dot(scaled, wcat[l], preferred_element_type=jnp.float32)[0:seqs]
        high = squares.astype(jnp.bfloat16).astype(jnp.float32)
        rest = squares - high
        mid = rest.astype(jnp.bfloat16).astype(jnp.float32)
        low = rest - mid
        y = jnp.where(lane == 192, high, y)
        y = jnp.where(lane == 193, mid, y)
        y = jnp.where(lane == 194, low, y)
        part_send[l, i] = y.astype(jnp.bfloat16)
        to = row_group(l, i)

        @pl.when(to != d)
        def _():
            part_copy(l, i, to).start()

    def gat_copy(l, i, peer):
        return pltpu.make_async_remote_copy(
            src_ref=gat.at[l, i],
            dst_ref=gat.at[l, i],
            send_sem=gat_send_sem.at[l],
            recv_sem=gat_sem.at[l, i],
            device_id={"dp": peer},
            device_id_type=MESH,
        )

    def update(l, i):
        @pl.when(row_group(l, i) == d)
        def _():
            pltpu.make_async_remote_copy(
                src_ref=part_recv.at[l],
                dst_ref=part_recv.at[l],
                send_sem=part_send_sem.at[l],
                recv_sem=part_sem.at[l],
                device_id={"tp": anti},
                device_id_type=MESH,
            ).wait_recv()
            total = part_send[l, i].astype(jnp.float32)
            for k in range(n_dp - 1):
                total += part_recv[l, k].astype(jnp.float32)
            squares = jnp.sum(total[:, 192:195], axis=1, keepdims=True)
            projected = total * lax.rsqrt(squares / D + epsilon)
            query_key = projected[:, 0:128]
            decay_pre = projected[:, 128:256]
            value = projected[:, 256:384]
            gate = projected[:, 384:512]
            log_sig = jnp.minimum(decay_pre, 0.0) - jnp.log1p(jnp.exp(-jnp.abs(decay_pre)))
            rate = jnp.exp(log_sig[:, 0:HEAD_KEY] / softness_factor + off_v[l])
            columns_qk = jnp.transpose(query_key, (1, 0))
            columns_rate = jnp.transpose(jnp.concatenate([rate, rate], axis=1), (1, 0))
            outs = []
            for s in range(seqs):
                q = columns_qk[0:HEAD_KEY, s : s + 1]
                k = columns_qk[HEAD_KEY : 2 * HEAD_KEY, s : s + 1] * HEAD_KEY ** (-0.5)
                r = columns_rate[0:HEAD_KEY, s : s + 1]
                fresh = r * st[l, s] + k * value[s : s + 1, :]
                st[l, s] = fresh
                outs.append(jnp.sum(q * fresh, axis=0, keepdims=True))
            readout = jnp.concatenate(outs, axis=0)
            normed = readout * lax.rsqrt(
                jnp.mean(readout * readout, axis=1, keepdims=True) + epsilon
            )
            normed = normed * ogain_v[l : l + 1, :]
            silu = gate / (1.0 + jnp.exp(-gate))
            gat[l, i] = (normed * silu).astype(jnp.bfloat16)

            def send(j, c):
                gat_copy(l, i, (d + 1 + j) % n_dp).start()
                return c

            lax.fori_loop(0, n_dp - 1, send, 0)
            pltpu.make_async_copy(st.at[l], new_state.at[l, :, 0], out_sem.at[l]).start()

    def reduce_copy(l, slot, owner):
        return pltpu.make_async_remote_copy(
            src_ref=rs_send.at[l, slot],
            dst_ref=rs_recv.at[l, (p - owner + n_tp) % n_tp - 1],
            send_sem=rs_send_sem.at[l],
            recv_sem=rs_sem.at[l],
            device_id={"tp": owner},
            device_id_type=MESH,
        )

    def out_project(l, i):
        @pl.when(row_group(l, i) != d)
        def _():
            gat_copy(l, i, row_group(l, i)).wait_recv()

        y = jnp.dot(gat[l, i], wout_v[l], preferred_element_type=jnp.float32)
        for j in range(members):
            pk[j, 0:1, 0:feats] = y[3 * j : 3 * j + 1]
            pk[j, 0:1, feats : feats + half] = y[3 * j + 1 : 3 * j + 2, 0:half]
            pk[j, 1:2, 0:half] = y[3 * j + 1 : 3 * j + 2, half:feats]
            pk[j, 1:2, half : half + feats] = y[3 * j + 2 : 3 * j + 3]
        base = source_group(i) * members + n_tp // 2
        for j in range(members):
            slot = members * i + j
            rs_send[l, slot] = pk[j].astype(jnp.bfloat16)
        for j in range(members):
            slot = members * i + j
            owner = (base + j) % n_tp

            @pl.when(owner != p)
            def _():
                reduce_copy(l, slot, owner).start()

    def loop(start, stop, fn):
        def step(i, c):
            fn(i)
            return c

        lax.fori_loop(start, stop, step, 0)

    lead = n_dp // 2
    for l in range(LAYERS):
        gather_start(l)

        def arrive(i):
            sg = source_group(i)
            gather_wait(l, sg, sg * members, members)
            project(l, i)

        gather_wait(l, group, 0, members - 1)
        project(l, 0)
        loop(1, lead, arrive)
        state_in[l].wait()

        def early(i):
            update(l, i)
            arrive(i + lead)

        def late(i):
            out_project(l, i)
            update(l, i + lead)

        loop(0, lead, early)
        loop(0, lead, late)
        loop(lead, n_dp, lambda i: out_project(l, i))

        pltpu.make_async_remote_copy(
            src_ref=rs_recv.at[l],
            dst_ref=rs_recv.at[l],
            send_sem=rs_send_sem.at[l],
            recv_sem=rs_sem.at[l],
            device_id={"tp": anti},
            device_id_type=MESH,
        ).wait_recv()
        total = rs_send[l, members * (n_dp - 1) + place].astype(jnp.float32)
        total += jnp.sum(rs_recv[l].astype(jnp.float32), axis=0)
        result = (total + ag[l, anti].astype(jnp.float32)).astype(jnp.bfloat16)
        if l + 1 < LAYERS:
            ag[l + 1, p] = result
        else:
            b = result.astype(jnp.float32)
            xs[0:1, :] = b[0:1, 0:feats]
            xs[1:2, 0:half] = b[0:1, feats : feats + half]
            xs[1:2, half:feats] = b[1:2, 0:half]
            xs[2:3, :] = b[1:2, half : half + feats]
            hidden_out[...] = xs[0:rows, :].astype(jnp.bfloat16)

    for l in range(LAYERS):
        for buf, sem, count in (
            (rs_recv, rs_send_sem, n_tp - 1),
            (part_recv, part_send_sem, n_dp - 1),
        ):
            ref = buf.at[l]
            pltpu.make_async_remote_copy(
                src_ref=ref, dst_ref=ref, send_sem=sem.at[l], recv_sem=rs_sem.at[l],
                device_id={"tp": anti}, device_id_type=MESH,
            ).wait_send()
        for buf, sem, count in (
            (ag, ag_send_sem, n_tp - 1),
            (gat, gat_send_sem, n_dp - 1),
        ):
            ref = buf.at[l, pl.ds(0, count)]
            pltpu.make_async_remote_copy(
                src_ref=ref, dst_ref=ref, send_sem=sem.at[l], recv_sem=rs_sem.at[l],
                device_id={"tp": anti}, device_id_type=MESH,
            ).wait_send()
        pltpu.make_async_copy(st.at[l], new_state.at[l, :, 0], out_sem.at[l]).wait()


def per_device(n_tp, n_dp, *args):
    hidden, state = args[0], args[10]
    rows, feats = hidden.shape
    members = n_tp // n_dp
    seqs = state.shape[1]
    block = (2, rows * feats // 2)
    any_spec = pl.BlockSpec(memory_space=pl.ANY)
    bf16, f32 = jnp.bfloat16, jnp.float32
    cols = 512
    dma = pltpu.SemaphoreType.DMA
    return pl.pallas_call(
        functools.partial(kernel, n_tp, n_dp),
        name="decode",
        out_shape=(
            jax.ShapeDtypeStruct(hidden.shape, hidden.dtype),
            jax.ShapeDtypeStruct(state.shape, state.dtype),
        ),
        in_specs=[any_spec] * 11,
        out_specs=(pl.BlockSpec(memory_space=pltpu.VMEM), any_spec),
        scratch_shapes=[
            pltpu.VMEM(hidden.shape, bf16),
            pltpu.VMEM(args[1].shape, f32),
            pltpu.VMEM((3,) + args[2].shape, bf16),
            pltpu.VMEM((LAYERS, feats, cols), bf16),
            pltpu.VMEM(args[7].shape, f32),
            pltpu.VMEM(args[8].shape, bf16),
            pltpu.VMEM(args[9].shape, f32),
            pltpu.VMEM((LAYERS, seqs) + state.shape[3:], f32),
            pltpu.VMEM((LAYERS, n_tp) + block, bf16),
            pltpu.VMEM((LAYERS, n_dp, seqs, cols), bf16),
            pltpu.VMEM((LAYERS, n_dp - 1, seqs, cols), bf16),
            pltpu.VMEM((LAYERS, n_dp, seqs, VALUE_CHANNELS), bf16),
            pltpu.VMEM((LAYERS, n_tp) + block, bf16),
            pltpu.VMEM((LAYERS, n_tp - 1) + block, bf16),
            pltpu.VMEM((16, feats), f32),
            pltpu.VMEM((members,) + block, f32),
            dma((10,)),
            dma((LAYERS,)),
            dma((LAYERS,)),
            dma((LAYERS,)),
            dma((LAYERS, n_dp)),
            dma((LAYERS,)),
            dma((LAYERS,)),
            dma((LAYERS,)),
            dma((LAYERS, n_dp)),
            dma((LAYERS,)),
            dma((LAYERS,)),
        ],
        compiler_params=pltpu.CompilerParams(
            collective_id=0, has_side_effects=True, vmem_limit_bytes=32 * 1024 * 1024
        ),
    )(*args)


def solution(mesh):
    return jax.shard_map(
        functools.partial(per_device, mesh.shape["tp"], mesh.shape["dp"]),
        mesh=mesh,
        in_specs=(
            P(("grp", "tp"), "dp"),
            P(None, "dp"),
            P(None, "dp", "tp"),
            P(None, "dp", "tp"),
            P(None, "dp", "tp"),
            P(None, "dp", "tp"),
            P(None, "dp", "tp"),
            P(None, "tp"),
            P(None, "tp", "dp"),
            P(None, ("grp", "dp"), "tp"),
            P(None, ("grp", "dp"), "tp", None, None),
        ),
        out_specs=(P(("grp", "tp"), "dp"), P(None, ("grp", "dp"), "tp", None, None)),
        check_vma=False,
    )
```

```python
import functools

import jax
import jax.numpy as jnp
from jax import lax
from jax.experimental import pallas as pl
from jax.experimental.pallas import tpu as pltpu
from jax.sharding import PartitionSpec as P

D = 4096
HEAD_KEY = 64
VALUE_CHANNELS = 128
LAYERS = 2

epsilon = 1e-06
softness_factor = 16.0

MESH = pl.DeviceIdType.MESH


def kernel(
    n_tp,
    n_dp,
    hidden,
    gain,
    w_query,
    w_key,
    w_decay,
    w_value,
    w_gate,
    out_gain,
    w_out,
    decay_offset,
    state,
    hidden_out,
    new_state,
    h_v,
    gain_v,
    wqkd,
    wvg,
    ogain_v,
    wout_v,
    off_v,
    st,
    ag,
    part_send,
    part_recv,
    gat,
    rs_send,
    rs_recv,
    xs,
    pk,
    local_sem,
    state_sem,
    out_sem,
    ag_send_sem,
    ag_sem,
    part_send_sem,
    part_sem,
    gat_send_sem,
    gat_sem,
    rs_send_sem,
    rs_sem,
):
    rows, feats = h_v.shape
    half = feats // 2
    members = n_tp // n_dp
    seqs = rows * members
    p = lax.axis_index("tp")
    d = lax.axis_index("dp")
    group = p // members
    place = p % members
    anti = (p + n_tp // 2) % n_tp
    near_first = jnp.where(2 * place >= members, 1, -1)

    barrier = pltpu.get_barrier_semaphore()

    def greet_tp(i, c):
        pl.semaphore_signal(
            barrier, inc=1, device_id={"tp": (p + 1 + i) % n_tp}, device_id_type=MESH
        )
        return c

    def greet_dp(i, c):
        pl.semaphore_signal(
            barrier, inc=1, device_id={"dp": (d + 1 + i) % n_dp}, device_id_type=MESH
        )
        return c

    lax.fori_loop(0, n_tp - 1, greet_tp, 0)
    lax.fori_loop(0, n_dp - 1, greet_dp, 0)

    fetches = [
        pltpu.make_async_copy(hidden, h_v, local_sem.at[0]),
        pltpu.make_async_copy(gain, gain_v, local_sem.at[1]),
        pltpu.make_async_copy(w_query, wqkd.at[:, pl.ds(0, HEAD_KEY)], local_sem.at[2]),
        pltpu.make_async_copy(w_key, wqkd.at[:, pl.ds(HEAD_KEY, HEAD_KEY)], local_sem.at[3]),
        pltpu.make_async_copy(w_decay, wqkd.at[:, pl.ds(2 * HEAD_KEY, HEAD_KEY)], local_sem.at[4]),
        pltpu.make_async_copy(w_value, wvg.at[:, :, pl.ds(0, 128)], local_sem.at[5]),
        pltpu.make_async_copy(w_gate, wvg.at[:, :, pl.ds(128, 128)], local_sem.at[6]),
        pltpu.make_async_copy(out_gain, ogain_v, local_sem.at[7]),
        pltpu.make_async_copy(w_out, wout_v, local_sem.at[8]),
        pltpu.make_async_copy(decay_offset, off_v, local_sem.at[9]),
    ]
    for f in fetches:
        f.start()
    state_in = [
        pltpu.make_async_copy(state.at[l, :, 0], st.at[l], state_sem.at[l]) for l in range(LAYERS)
    ]
    for f in state_in:
        f.start()
    fetches[0].wait()
    xs[...] = jnp.zeros_like(xs)

    first = h_v[...].astype(jnp.float32)
    pk[0, 0:1, 0:feats] = first[0:1]
    pk[0, 0:1, feats : feats + half] = first[1:2, 0:half]
    pk[0, 1:2, 0:half] = first[1:2, half:feats]
    pk[0, 1:2, half : half + feats] = first[2:3]
    ag[0, p] = pk[0].astype(jnp.bfloat16)

    wqkd[:, 3 * HEAD_KEY :, :] = jnp.zeros_like(wqkd[:, 3 * HEAD_KEY :, :])

    pl.semaphore_wait(barrier, n_tp - 1 + n_dp - 1)

    def source_group(i):
        k = (i + 1) // 2
        side = jnp.where(i % 2 == 1, near_first, -near_first)
        return (group + n_dp + side * k) % n_dp

    def row_group(l, i):
        return (source_group(i) + l * (n_dp // 2)) % n_dp

    def gather_copy(l, peer):
        return pltpu.make_async_remote_copy(
            src_ref=ag.at[l, p],
            dst_ref=ag.at[l, p],
            send_sem=ag_send_sem.at[l],
            recv_sem=ag_sem.at[l, group],
            device_id={"tp": peer},
            device_id_type=MESH,
        )

    def gather_start(l):
        def one(i, c):
            k = n_tp // 2 - (i + 1) // 2
            off = jnp.where(i % 2 == 1, k, n_tp - k)
            gather_copy(l, (p + off) % n_tp).start()
            return c

        lax.fori_loop(0, n_tp - 1, one, 0)

    def gather_wait(l, sg, first_slot, count):
        block = ag.at[l, pl.ds(first_slot, count)]
        pltpu.make_async_remote_copy(
            src_ref=block,
            dst_ref=block,
            send_sem=ag_send_sem.at[l],
            recv_sem=ag_sem.at[l, sg],
            device_id={"tp": anti},
            device_id_type=MESH,
        ).wait_recv()

    def part_copy(l, i, to):
        slot = (d - to + n_dp) % n_dp - 1
        return pltpu.make_async_remote_copy(
            src_ref=part_send.at[l, i],
            dst_ref=part_recv.at[l, slot],
            send_sem=part_send_sem.at[l],
            recv_sem=part_sem.at[l],
            device_id={"dp": to},
            device_id_type=MESH,
        )

    lane = lax.broadcasted_iota(jnp.int32, (seqs, 512), 1)

    def project(l, i):
        sg = source_group(i)
        for j in range(members):
            b = ag[l, sg * members + j].astype(jnp.float32)
            xs[3 * j : 3 * j + 1, :] = b[0:1, 0:feats]
            xs[3 * j + 1 : 3 * j + 2, 0:half] = b[0:1, feats : feats + half]
            xs[3 * j + 1 : 3 * j + 2, half:feats] = b[1:2, 0:half]
            xs[3 * j + 2 : 3 * j + 3, :] = b[1:2, half : half + feats]
        x = xs[...]
        squares = jnp.sum(x * x, axis=1, keepdims=True)[0:seqs]
        scaled = (x * gain_v[l : l + 1, :]).astype(jnp.bfloat16)
        y = jnp.concatenate(
            [
                lax.dot_general(
                    scaled,
                    wqkd[l],
                    (((1,), (1,)), ((), ())),
                    preferred_element_type=jnp.float32,
                ),
                jnp.dot(scaled, wvg[l], preferred_element_type=jnp.float32),
            ],
            axis=1,
        )[0:seqs]
        high = squares.astype(jnp.bfloat16).astype(jnp.float32)
        rest = squares - high
        mid = rest.astype(jnp.bfloat16).astype(jnp.float32)
        low = rest - mid
        y = jnp.where(lane == 192, high, y)
        y = jnp.where(lane == 193, mid, y)
        y = jnp.where(lane == 194, low, y)
        part_send[l, i] = y.astype(jnp.bfloat16)
        to = row_group(l, i)

        @pl.when(to != d)
        def _():
            part_copy(l, i, to).start()

    def gat_copy(l, i, peer):
        return pltpu.make_async_remote_copy(
            src_ref=gat.at[l, i],
            dst_ref=gat.at[l, i],
            send_sem=gat_send_sem.at[l],
            recv_sem=gat_sem.at[l, i],
            device_id={"dp": peer},
            device_id_type=MESH,
        )

    def update(l, i):
        @pl.when(row_group(l, i) == d)
        def _():
            pltpu.make_async_remote_copy(
                src_ref=part_recv.at[l],
                dst_ref=part_recv.at[l],
                send_sem=part_send_sem.at[l],
                recv_sem=part_sem.at[l],
                device_id={"tp": anti},
                device_id_type=MESH,
            ).wait_recv()
            total = part_send[l, i].astype(jnp.float32)
            for k in range(n_dp - 1):
                total += part_recv[l, k].astype(jnp.float32)
            squares = jnp.sum(total[:, 192:195], axis=1, keepdims=True)
            projected = total * lax.rsqrt(squares / D + epsilon)
            query_key = projected[:, 0:128]
            decay_pre = projected[:, 128:256]
            value = projected[:, 256:384]
            gate = projected[:, 384:512]
            log_sig = jnp.minimum(decay_pre, 0.0) - jnp.log1p(jnp.exp(-jnp.abs(decay_pre)))
            rate = jnp.exp(log_sig[:, 0:HEAD_KEY] / softness_factor + off_v[:, l, :])
            columns_qk = jnp.transpose(query_key, (1, 0))
            columns_rate = jnp.transpose(jnp.concatenate([rate, rate], axis=1), (1, 0))
            outs = []
            for s in range(seqs):
                q = columns_qk[0:HEAD_KEY, s : s + 1]
                k = columns_qk[HEAD_KEY : 2 * HEAD_KEY, s : s + 1] * HEAD_KEY ** (-0.5)
                r = columns_rate[0:HEAD_KEY, s : s + 1]
                fresh = r * st[l, s] + k * value[s : s + 1, :]
                st[l, s] = fresh
                outs.append(jnp.sum(q * fresh, axis=0, keepdims=True))
            readout = jnp.concatenate(outs, axis=0)
            normed = readout * lax.rsqrt(
                jnp.mean(readout * readout, axis=1, keepdims=True) + epsilon
            )
            normed = normed * ogain_v[l : l + 1, :]
            silu = gate / (1.0 + jnp.exp(-gate))
            gat[l, i] = (normed * silu).astype(jnp.bfloat16)

            def send(j, c):
                gat_copy(l, i, (d + 1 + j) % n_dp).start()
                return c

            lax.fori_loop(0, n_dp - 1, send, 0)
            pltpu.make_async_copy(st.at[l], new_state.at[l, :, 0], out_sem.at[l]).start()

    def reduce_copy(l, slot, owner):
        return pltpu.make_async_remote_copy(
            src_ref=rs_send.at[l, slot],
            dst_ref=rs_recv.at[l, (p - owner + n_tp) % n_tp - 1],
            send_sem=rs_send_sem.at[l],
            recv_sem=rs_sem.at[l],
            device_id={"tp": owner},
            device_id_type=MESH,
        )

    def out_project(l, i):
        @pl.when(row_group(l, i) != d)
        def _():
            gat_copy(l, i, row_group(l, i)).wait_recv()

        y = jnp.dot(gat[l, i], wout_v[l], preferred_element_type=jnp.float32)
        for j in range(members):
            pk[j, 0:1, 0:feats] = y[3 * j : 3 * j + 1]
            pk[j, 0:1, feats : feats + half] = y[3 * j + 1 : 3 * j + 2, 0:half]
            pk[j, 1:2, 0:half] = y[3 * j + 1 : 3 * j + 2, half:feats]
            pk[j, 1:2, half : half + feats] = y[3 * j + 2 : 3 * j + 3]
        base = source_group(i) * members + n_tp // 2
        for j in range(members):
            slot = members * i + j
            rs_send[l, slot] = pk[j].astype(jnp.bfloat16)
        for j in range(members):
            slot = members * i + j
            owner = (base + j) % n_tp

            @pl.when(owner != p)
            def _():
                reduce_copy(l, slot, owner).start()

    def loop(start, stop, fn):
        def step(i, c):
            fn(i)
            return c

        lax.fori_loop(start, stop, step, 0)

    lead = n_dp // 2
    for l in range(LAYERS):
        gather_start(l)
        if l == 0:
            for f in fetches[1:]:
                f.wait()

        def arrive(i):
            sg = source_group(i)
            gather_wait(l, sg, sg * members, members)
            project(l, i)

        gather_wait(l, group, 0, members - 1)
        project(l, 0)
        loop(1, lead, arrive)
        state_in[l].wait()

        def early(i):
            update(l, i)
            arrive(i + lead)

        def late(i):
            out_project(l, i)
            update(l, i + lead)

        loop(0, lead, early)
        loop(0, lead, late)
        loop(lead, n_dp, lambda i: out_project(l, i))

        pltpu.make_async_remote_copy(
            src_ref=rs_recv.at[l],
            dst_ref=rs_recv.at[l],
            send_sem=rs_send_sem.at[l],
            recv_sem=rs_sem.at[l],
            device_id={"tp": anti},
            device_id_type=MESH,
        ).wait_recv()
        total = rs_send[l, members * (n_dp - 1) + place].astype(jnp.float32)
        total += jnp.sum(rs_recv[l].astype(jnp.float32), axis=0)
        result = (total + ag[l, anti].astype(jnp.float32)).astype(jnp.bfloat16)
        if l + 1 < LAYERS:
            ag[l + 1, p] = result
        else:
            b = result.astype(jnp.float32)
            xs[0:1, :] = b[0:1, 0:feats]
            xs[1:2, 0:half] = b[0:1, feats : feats + half]
            xs[1:2, half:feats] = b[1:2, 0:half]
            xs[2:3, :] = b[1:2, half : half + feats]
            hidden_out[...] = xs[0:rows, :].astype(jnp.bfloat16)

    for l in range(LAYERS):
        for buf, sem, count in (
            (rs_recv, rs_send_sem, n_tp - 1),
            (part_recv, part_send_sem, n_dp - 1),
        ):
            ref = buf.at[l]
            pltpu.make_async_remote_copy(
                src_ref=ref, dst_ref=ref, send_sem=sem.at[l], recv_sem=rs_sem.at[l],
                device_id={"tp": anti}, device_id_type=MESH,
            ).wait_send()
        for buf, sem, count in (
            (ag, ag_send_sem, n_tp - 1),
            (gat, gat_send_sem, n_dp - 1),
        ):
            ref = buf.at[l, pl.ds(0, count)]
            pltpu.make_async_remote_copy(
                src_ref=ref, dst_ref=ref, send_sem=sem.at[l], recv_sem=rs_sem.at[l],
                device_id={"tp": anti}, device_id_type=MESH,
            ).wait_send()
        pltpu.make_async_copy(st.at[l], new_state.at[l, :, 0], out_sem.at[l]).wait()


def per_device(n_tp, n_dp, *args):
    hidden, state = args[0], args[10]
    rows, feats = hidden.shape
    members = n_tp // n_dp
    seqs = state.shape[1]
    block = (2, rows * feats // 2)
    hbm_spec = pl.BlockSpec(memory_space=pltpu.HBM)
    vmem_spec = pl.BlockSpec(memory_space=pltpu.VMEM)
    args = list(args)
    for i in (2, 3, 4):
        args[i] = jnp.swapaxes(args[i], 1, 2)
    args[9] = jnp.swapaxes(args[9], 0, 1)
    bf16, f32 = jnp.bfloat16, jnp.float32
    cols = 512
    dma = pltpu.SemaphoreType.DMA
    return pl.pallas_call(
        functools.partial(kernel, n_tp, n_dp),
        name="decode",
        out_shape=(
            jax.ShapeDtypeStruct(hidden.shape, hidden.dtype),
            jax.ShapeDtypeStruct(state.shape, state.dtype),
        ),
        in_specs=[hbm_spec] * 11,
        out_specs=(vmem_spec, hbm_spec),
        scratch_shapes=[
            pltpu.VMEM(hidden.shape, bf16),
            pltpu.VMEM(args[1].shape, f32),
            pltpu.VMEM((LAYERS, 4 * HEAD_KEY, feats), bf16),
            pltpu.VMEM((LAYERS, feats, 2 * VALUE_CHANNELS), bf16),
            pltpu.VMEM(args[7].shape, f32),
            pltpu.VMEM(args[8].shape, bf16),
            pltpu.VMEM(args[9].shape, f32),
            pltpu.VMEM((LAYERS, seqs) + state.shape[3:], f32),
            pltpu.VMEM((LAYERS, n_tp) + block, bf16),
            pltpu.VMEM((LAYERS, n_dp, seqs, cols), bf16),
            pltpu.VMEM((LAYERS, n_dp - 1, seqs, cols), bf16),
            pltpu.VMEM((LAYERS, n_dp, seqs, VALUE_CHANNELS), bf16),
            pltpu.VMEM((LAYERS, n_tp) + block, bf16),
            pltpu.VMEM((LAYERS, n_tp - 1) + block, bf16),
            pltpu.VMEM((16, feats), f32),
            pltpu.VMEM((members,) + block, f32),
            dma((10,)),
            dma((LAYERS,)),
            dma((LAYERS,)),
            dma((LAYERS,)),
            dma((LAYERS, n_dp)),
            dma((LAYERS,)),
            dma((LAYERS,)),
            dma((LAYERS,)),
            dma((LAYERS, n_dp)),
            dma((LAYERS,)),
            dma((LAYERS,)),
        ],
        compiler_params=pltpu.CompilerParams(
            collective_id=0, has_side_effects=True, vmem_limit_bytes=64000000
        ),
    )(*args)


def solution(mesh):
    return jax.shard_map(
        functools.partial(per_device, mesh.shape["tp"], mesh.shape["dp"]),
        mesh=mesh,
        in_specs=(
            P(("grp", "tp"), "dp"),
            P(None, "dp"),
            P(None, "dp", "tp"),
            P(None, "dp", "tp"),
            P(None, "dp", "tp"),
            P(None, "dp", "tp"),
            P(None, "dp", "tp"),
            P(None, "tp"),
            P(None, "tp", "dp"),
            P(None, ("grp", "dp"), "tp"),
            P(None, ("grp", "dp"), "tp", None, None),
        ),
        out_specs=(P(("grp", "tp"), "dp"), P(None, ("grp", "dp"), "tp", None, None)),
        check_vma=False,
    )
```

```python
import functools

import jax
import jax.numpy as jnp
from jax import lax
from jax.experimental import pallas as pl
from jax.experimental.pallas import tpu as pltpu
from jax.sharding import PartitionSpec as P

D = 4096
HEAD_KEY = 64
VALUE_CHANNELS = 128
LAYERS = 2

epsilon = 1e-06
softness_factor = 16.0

MESH = pl.DeviceIdType.MESH


def kernel(
    n_tp,
    n_dp,
    hidden,
    gain,
    w_query,
    w_key,
    w_decay,
    w_value,
    w_gate,
    out_gain,
    w_out,
    decay_offset,
    state,
    hidden_out,
    new_state,
    h_v,
    gain_v,
    wqkd,
    wvg,
    ogain_v,
    wout_v,
    off_v,
    st,
    ag,
    part_send,
    part_recv,
    gat,
    terms,
    terms_in,
    sums,
    sums_in,
    xs,
    pk,
    local_sem,
    state_sem,
    far_send_sem,
    far_sem,
    mate_send_sem,
    mate_sem,
    part_send_sem,
    part_sem,
    gat_send_sem,
    gat_sem,
    terms_send_sem,
    terms_sem,
    sums_send_sem,
    sums_sem,
):
    rows, feats = h_v.shape
    half = feats // 2
    members = n_tp // n_dp
    seqs = rows * members
    p = lax.axis_index("tp")
    d = lax.axis_index("dp")
    group = p // members
    place = p % members
    anti = (p + n_tp // 2) % n_tp
    last = n_dp - 1

    def mate(j):
        return group * members + (place + 1 + j) % members

    barrier = pltpu.get_barrier_semaphore()
    greeted = [{"tp": mate(j)} for j in range(members - 1)]
    greeted += [{"tp": (p + members) % n_tp}, {"tp": (p - members + n_tp) % n_tp}]
    greeted += [{"dp": (d + 1 + j) % n_dp} for j in range(n_dp - 1)]
    for device in greeted:
        pl.semaphore_signal(barrier, inc=1, device_id=device, device_id_type=MESH)

    fetches = [
        pltpu.make_async_copy(hidden, h_v, local_sem.at[0]),
        pltpu.make_async_copy(gain, gain_v, local_sem.at[1]),
        pltpu.make_async_copy(w_query, wqkd.at[:, pl.ds(0, HEAD_KEY)], local_sem.at[2]),
        pltpu.make_async_copy(w_key, wqkd.at[:, pl.ds(HEAD_KEY, HEAD_KEY)], local_sem.at[3]),
        pltpu.make_async_copy(w_decay, wqkd.at[:, pl.ds(2 * HEAD_KEY, HEAD_KEY)], local_sem.at[4]),
        pltpu.make_async_copy(w_value, wvg.at[:, :, pl.ds(0, 128)], local_sem.at[5]),
        pltpu.make_async_copy(w_gate, wvg.at[:, :, pl.ds(128, 128)], local_sem.at[6]),
        pltpu.make_async_copy(out_gain, ogain_v, local_sem.at[7]),
        pltpu.make_async_copy(w_out, wout_v, local_sem.at[8]),
        pltpu.make_async_copy(decay_offset, off_v, local_sem.at[9]),
    ]
    for f in fetches:
        f.start()
    state_in = [
        pltpu.make_async_copy(state.at[l, :, 0], st.at[l], state_sem.at[l]) for l in range(LAYERS)
    ]
    for f in state_in:
        f.start()

    xs[...] = jnp.zeros_like(xs)
    wqkd[:, 3 * HEAD_KEY :, :] = jnp.zeros_like(wqkd[:, 3 * HEAD_KEY :, :])

    fetches[0].wait()
    first = h_v[...].astype(jnp.float32)
    pk[0, 0:1, 0:feats] = first[0:1]
    pk[0, 0:1, feats : feats + half] = first[1:2, 0:half]
    pk[0, 1:2, 0:half] = first[1:2, half:feats]
    pk[0, 1:2, half : half + feats] = first[2:3]
    ag[0, p] = pk[0].astype(jnp.bfloat16)

    with jax.named_scope("barrier"):
        pl.semaphore_wait(barrier, len(greeted))

    def offset(i):
        k = (i + 1) // 2
        return jnp.where(i % 2 == 1, n_dp - k, k)

    def source_group(i):
        return (group + offset(i)) % n_dp

    def row_group(l, i):
        return (source_group(i) + l * (n_dp // 2)) % n_dp

    def source(i):
        return source_group(i) * members + place

    def remote(src, dst, send_sem, recv_sem, device):
        return pltpu.make_async_remote_copy(
            src_ref=src,
            dst_ref=dst,
            send_sem=send_sem,
            recv_sem=recv_sem,
            device_id=device,
            device_id_type=MESH,
        )

    def arrived(ref, sem):
        remote(ref, ref, far_send_sem.at[0], sem, {"tp": anti}).wait_recv()

    def far_copy(l, sigma, i, to):
        return remote(
            ag.at[l, sigma], ag.at[l, sigma], far_send_sem.at[l], far_sem.at[l, i], {"tp": to}
        )

    def up(k):
        return (p + members * k) % n_tp

    def down(k):
        return (p - members * k + n_tp) % n_tp

    def to_mates(l, i):
        sigma = source(i)
        for j in range(members - 1):
            remote(
                ag.at[l, sigma],
                ag.at[l, sigma],
                mate_send_sem.at[l],
                mate_sem.at[l, i],
                {"tp": mate(j)},
            ).start()

    def begin(l):
        if l == 0:
            far_copy(l, p, 1, up(1)).start()
            far_copy(l, p, 2, down(1)).start()
        else:
            for k in range(n_dp // 2, 0, -1):
                far_copy(l, p, 2 * k - 1, up(k)).start()
                if 2 * k < n_dp:
                    far_copy(l, p, 2 * k, down(k)).start()
        to_mates(l, 0)

    def forward(l, i):
        sigma = source(i)
        arrived(ag.at[l, sigma], far_sem.at[l, i])
        if l == 0:

            @pl.when(i + 2 < n_dp)
            def _():
                far_copy(l, sigma, i + 2, jnp.where(i % 2 == 1, up(1), down(1))).start()

        to_mates(l, i)

    lane = lax.broadcasted_iota(jnp.int32, (seqs, 512), 1)

    def project(l, i):
        sg = source_group(i)
        arrived(ag.at[l, pl.ds(0, members - 1)], mate_sem.at[l, i])
        for j in range(members):
            b = ag[l, sg * members + j].astype(jnp.float32)
            xs[3 * j : 3 * j + 1, :] = b[0:1, 0:feats]
            xs[3 * j + 1 : 3 * j + 2, 0:half] = b[0:1, feats : feats + half]
            xs[3 * j + 1 : 3 * j + 2, half:feats] = b[1:2, 0:half]
            xs[3 * j + 2 : 3 * j + 3, :] = b[1:2, half : half + feats]
        x = xs[...]
        squares = jnp.sum(x * x, axis=1, keepdims=True)[0:seqs]
        scaled = (x * gain_v[l : l + 1, :]).astype(jnp.bfloat16)
        y = jnp.concatenate(
            [
                lax.dot_general(
                    scaled,
                    wqkd[l],
                    (((1,), (1,)), ((), ())),
                    preferred_element_type=jnp.float32,
                ),
                jnp.dot(scaled, wvg[l], preferred_element_type=jnp.float32),
            ],
            axis=1,
        )[0:seqs]
        high = squares.astype(jnp.bfloat16).astype(jnp.float32)
        rest = squares - high
        mid = rest.astype(jnp.bfloat16).astype(jnp.float32)
        low = rest - mid
        y = jnp.where(lane == 192, high, y)
        y = jnp.where(lane == 193, mid, y)
        y = jnp.where(lane == 194, low, y)
        part_send[l, i] = y.astype(jnp.bfloat16)
        to = row_group(l, i)

        @pl.when(to != d)
        def _():
            slot = (d - to + n_dp) % n_dp - 1
            remote(
                part_send.at[l, i],
                part_recv.at[l, slot],
                part_send_sem.at[l],
                part_sem.at[l],
                {"dp": to},
            ).start()

    def gat_copy(l, i, peer):
        return remote(
            gat.at[l, i], gat.at[l, i], gat_send_sem.at[l], gat_sem.at[l, i], {"dp": peer}
        )

    def update(l, i):
        arrived(part_recv.at[l], part_sem.at[l])
        total = part_send[l, i].astype(jnp.float32)
        for k in range(n_dp - 1):
            total += part_recv[l, k].astype(jnp.float32)
        squares = jnp.sum(total[:, 192:195], axis=1, keepdims=True)
        projected = total * lax.rsqrt(squares / D + epsilon)
        query_key = projected[:, 0:128]
        decay_pre = projected[:, 128:256]
        value = projected[:, 256:384]
        gate = projected[:, 384:512]
        log_sig = jnp.minimum(decay_pre, 0.0) - jnp.log1p(jnp.exp(-jnp.abs(decay_pre)))
        rate = jnp.exp(log_sig[:, 0:HEAD_KEY] / softness_factor + off_v[:, l, :])
        columns_qk = jnp.transpose(query_key, (1, 0))
        columns_rate = jnp.transpose(jnp.concatenate([rate, rate], axis=1), (1, 0))
        outs = []
        for s in range(seqs):
            q = columns_qk[0:HEAD_KEY, s : s + 1]
            k = columns_qk[HEAD_KEY : 2 * HEAD_KEY, s : s + 1] * HEAD_KEY ** (-0.5)
            r = columns_rate[0:HEAD_KEY, s : s + 1]
            fresh = r * st[l, s] + k * value[s : s + 1, :]
            new_state[l, s, 0] = fresh
            outs.append(jnp.sum(q * fresh, axis=0, keepdims=True))
        readout = jnp.concatenate(outs, axis=0)
        normed = readout * lax.rsqrt(jnp.mean(readout * readout, axis=1, keepdims=True) + epsilon)
        normed = normed * ogain_v[l : l + 1, :]
        silu = gate / (1.0 + jnp.exp(-gate))
        gat[l, i] = (normed * silu).astype(jnp.bfloat16)
        for j in range(n_dp - 1):
            gat_copy(l, i, (d + 1 + j) % n_dp).start()

    def out_project(l, i):
        @pl.when(row_group(l, i) != d)
        def _():
            arrived(gat.at[l, i], gat_sem.at[l, i])

        y = jnp.dot(gat[l, i], wout_v[l], preferred_element_type=jnp.float32)
        for j in range(members):
            pk[j, 0:1, 0:feats] = y[3 * j : 3 * j + 1]
            pk[j, 0:1, feats : feats + half] = y[3 * j + 1 : 3 * j + 2, 0:half]
            pk[j, 1:2, 0:half] = y[3 * j + 1 : 3 * j + 2, half:feats]
            pk[j, 1:2, half : half + feats] = y[3 * j + 2 : 3 * j + 3]
        for j in range(members):
            terms[l, members * i + j] = pk[j].astype(jnp.bfloat16)
        for j in range(members - 1):
            to = (place + 1 + j) % members
            remote(
                terms.at[l, members * i + to],
                terms_in.at[l, (members - 1) * i + members - 2 - j],
                terms_send_sem.at[l],
                terms_sem.at[l, i],
                {"tp": mate(j)},
            ).start()

    def add_quad(l, i):
        arrived(terms_in.at[l, pl.ds(0, members - 1)], terms_sem.at[l, i])
        total = terms[l, members * i + place].astype(jnp.float32)
        for j in range(members - 1):
            total += terms_in[l, (members - 1) * i + j].astype(jnp.float32)
        sums[l, i] = total.astype(jnp.bfloat16)

        @pl.when(i < last)
        def _():
            remote(
                sums.at[l, i],
                sums_in.at[l, i],
                sums_send_sem.at[l],
                sums_sem.at[l],
                {"tp": (source(i) + n_tp // 2) % n_tp},
            ).start()

    def both(fn, l, k):
        for i in (2 * k - 1, 2 * k):

            @pl.when((i >= 0) & (i < n_dp))
            def _():
                fn(l, i)

    def mine(l, k):
        low, high = 2 * k - 1, 2 * k
        at_low = (low >= 0) & (low < n_dp) & (row_group(l, jnp.maximum(low, 0)) == d)
        at_high = (high >= 0) & (high < n_dp) & (row_group(l, jnp.maximum(high, 0)) == d)

        @pl.when(at_low | at_high)
        def _():
            update(l, jnp.where(at_low, low, high))

    def far(l, k):
        @pl.when(k > 0)
        def _():
            both(forward, l, k)

    steps = n_dp // 2
    for l in range(LAYERS):
        begin(l)
        if l == 0:
            for f in fetches[1:]:
                f.wait()
        state_in[l].wait()

        def tick(t, c):
            if l == 0:
                both(project, l, t - 1)
                mine(l, t - 2)
                far(l, t)
                both(out_project, l, t - 3)
                both(add_quad, l, t - 4)
            else:
                far(l, t)
                both(project, l, t - 1)
                both(add_quad, l, t - 5)
                both(out_project, l, t - 4)
                mine(l, t - 2)
            return c

        lax.fori_loop(1, steps + (5 if l == 0 else 6), tick, 0)

        with jax.named_scope("owner_wait"):
            arrived(sums_in.at[l], sums_sem.at[l])
        total = sums[l, last].astype(jnp.float32)
        total += jnp.sum(sums_in[l].astype(jnp.float32), axis=0)
        result = (total + ag[l, anti].astype(jnp.float32)).astype(jnp.bfloat16)
        if l + 1 < LAYERS:
            ag[l + 1, p] = result
        else:
            b = result.astype(jnp.float32)
            xs[0:1, :] = b[0:1, 0:feats]
            xs[1:2, 0:half] = b[0:1, feats : feats + half]
            xs[1:2, half:feats] = b[1:2, 0:half]
            xs[2:3, :] = b[1:2, half : half + feats]
            hidden_out[...] = xs[0:rows, :].astype(jnp.bfloat16)

    for l in range(LAYERS):
        many = (members - 1) * n_dp
        for ref, sem in (
            (sums_in.at[l], far_send_sem),
            (sums_in.at[l], sums_send_sem),
            (ag.at[l, pl.ds(0, many)], mate_send_sem),
            (ag.at[l, pl.ds(0, many)], terms_send_sem),
            (part_recv.at[l], part_send_sem),
            (gat.at[l, pl.ds(0, n_dp - 1)], gat_send_sem),
        ):
            remote(ref, ref, sem.at[l], part_sem.at[l], {"tp": anti}).wait_send()


def store_results(h, s, h_out, s_out, sem):
    copies = [
        pltpu.make_async_copy(s, s_out, sem.at[0]),
        pltpu.make_async_copy(h, h_out, sem.at[1]),
    ]
    for c in copies:
        c.start()
    for c in copies:
        c.wait()


def per_device(n_tp, n_dp, *args):
    hidden, state = args[0], args[10]
    rows, feats = hidden.shape
    members = n_tp // n_dp
    seqs = state.shape[1]
    block = (2, rows * feats // 2)
    hbm_spec = pl.BlockSpec(memory_space=pltpu.HBM)
    vmem_spec = pl.BlockSpec(memory_space=pltpu.VMEM)
    args = list(args)
    for i in (2, 3, 4):
        args[i] = jnp.swapaxes(args[i], 1, 2)
    args[9] = jnp.swapaxes(args[9], 0, 1)
    bf16, f32 = jnp.bfloat16, jnp.float32
    cols = 512
    dma = pltpu.SemaphoreType.DMA
    results = pl.pallas_call(
        functools.partial(kernel, n_tp, n_dp),
        name="decode",
        out_shape=(
            pltpu.VMEM(hidden.shape, hidden.dtype),
            pltpu.VMEM(state.shape, state.dtype),
        ),
        in_specs=[hbm_spec] * 11,
        out_specs=(vmem_spec, vmem_spec),
        scratch_shapes=[
            pltpu.VMEM(hidden.shape, bf16),
            pltpu.VMEM(args[1].shape, f32),
            pltpu.VMEM((LAYERS, 4 * HEAD_KEY, feats), bf16),
            pltpu.VMEM((LAYERS, feats, 2 * VALUE_CHANNELS), bf16),
            pltpu.VMEM(args[7].shape, f32),
            pltpu.VMEM(args[8].shape, bf16),
            pltpu.VMEM(args[9].shape, f32),
            pltpu.VMEM((LAYERS, seqs) + state.shape[3:], f32),
            pltpu.VMEM((LAYERS, n_tp) + block, bf16),
            pltpu.VMEM((LAYERS, n_dp, seqs, cols), bf16),
            pltpu.VMEM((LAYERS, n_dp - 1, seqs, cols), bf16),
            pltpu.VMEM((LAYERS, n_dp, seqs, VALUE_CHANNELS), bf16),
            pltpu.VMEM((LAYERS, n_tp) + block, bf16),
            pltpu.VMEM((LAYERS, n_dp * (members - 1)) + block, bf16),
            pltpu.VMEM((LAYERS, n_dp) + block, bf16),
            pltpu.VMEM((LAYERS, n_dp - 1) + block, bf16),
            pltpu.VMEM((16, feats), f32),
            pltpu.VMEM((members,) + block, f32),
            dma((10,)),
            dma((LAYERS,)),
            dma((LAYERS,)),
            dma((LAYERS, n_dp)),
            dma((LAYERS,)),
            dma((LAYERS, n_dp)),
            dma((LAYERS,)),
            dma((LAYERS,)),
            dma((LAYERS,)),
            dma((LAYERS, n_dp)),
            dma((LAYERS,)),
            dma((LAYERS, n_dp)),
            dma((LAYERS,)),
            dma((LAYERS,)),
        ],
        compiler_params=pltpu.CompilerParams(
            collective_id=0, has_side_effects=True, vmem_limit_bytes=64000000
        ),
    )(*args)
    return pl.pallas_call(
        store_results,
        name="store_results",
        out_shape=tuple(jax.ShapeDtypeStruct(r.shape, r.dtype) for r in (hidden, state)),
        in_specs=[vmem_spec] * 2,
        out_specs=(hbm_spec, hbm_spec),
        scratch_shapes=[dma((2,))],
    )(*[pltpu.with_memory_space_constraint(r, pltpu.VMEM) for r in results])


def solution(mesh):
    return jax.shard_map(
        functools.partial(per_device, mesh.shape["tp"], mesh.shape["dp"]),
        mesh=mesh,
        in_specs=(
            P(("grp", "tp"), "dp"),
            P(None, "dp"),
            P(None, "dp", "tp"),
            P(None, "dp", "tp"),
            P(None, "dp", "tp"),
            P(None, "dp", "tp"),
            P(None, "dp", "tp"),
            P(None, "tp"),
            P(None, "tp", "dp"),
            P(None, ("grp", "dp"), "tp"),
            P(None, ("grp", "dp"), "tp", None, None),
        ),
        out_specs=(P(("grp", "tp"), "dp"), P(None, ("grp", "dp"), "tp", None, None)),
        check_vma=False,
    )
```

```python
import functools

import jax
import jax.numpy as jnp
from jax import lax
from jax.experimental import pallas as pl
from jax.experimental.pallas import tpu as pltpu
from jax.sharding import PartitionSpec as P

D = 4096
HEAD_KEY = 64
VALUE_CHANNELS = 128
LAYERS = 2

epsilon = 1e-06
softness_factor = 16.0

MESH = pl.DeviceIdType.MESH

STEPS = (
    (
        "A0", "F1", "F2", "A1", "F3", "A2", "U0", "A3",
        "F4", "U1", "O0", "U3", "U2", "A4", "O1", "O2",
        "U4", "O3", "O4",
    ),
    (
        "F1", "A0", "F2", "A1", "U0", "F3", "A2", "U1",
        "F4", "A3", "O0", "U2", "O1", "A4", "U3", "O2",
        "U4", "O3", "O4",
    ),
)


def kernel(
    n_tp,
    n_dp,
    hidden,
    gain,
    w_query,
    w_key,
    w_decay,
    w_value,
    w_gate,
    out_gain,
    w_out,
    decay_offset,
    state,
    hidden_out,
    new_state,
    h_v,
    gain_v,
    wqkd,
    wvg,
    ogain_v,
    wout_v,
    off_v,
    st,
    ag,
    part_send,
    part_recv,
    gat,
    terms,
    terms_in,
    xs,
    pk,
    local_sem,
    state_sem,
    far_send_sem,
    far_sem,
    mate_send_sem,
    mate_sem,
    part_send_sem,
    part_sem,
    gat_send_sem,
    gat_sem,
    terms_send_sem,
    terms_sem,
):
    rows, feats = h_v.shape
    half = feats // 2
    members = n_tp // n_dp
    seqs = rows * members
    p = lax.axis_index("tp")
    d = lax.axis_index("dp")
    group = p // members
    place = p % members
    anti = (p + n_tp // 2) % n_tp
    last = n_dp - 1

    def mate(j):
        return group * members + (place + 1 + j) % members

    barrier = pltpu.get_barrier_semaphore()
    greeted = [{"tp": mate(j)} for j in range(members - 1)]
    greeted += [{"tp": (p + members) % n_tp}, {"tp": (p - members + n_tp) % n_tp}]
    greeted += [{"dp": (d + 1 + j) % n_dp} for j in range(n_dp - 1)]
    for device in greeted:
        pl.semaphore_signal(barrier, inc=1, device_id=device, device_id_type=MESH)

    fetches = [
        pltpu.make_async_copy(hidden, h_v, local_sem.at[0]),
        pltpu.make_async_copy(gain, gain_v, local_sem.at[1]),
        pltpu.make_async_copy(w_query, wqkd.at[:, pl.ds(0, HEAD_KEY)], local_sem.at[2]),
        pltpu.make_async_copy(w_key, wqkd.at[:, pl.ds(HEAD_KEY, HEAD_KEY)], local_sem.at[3]),
        pltpu.make_async_copy(w_decay, wqkd.at[:, pl.ds(2 * HEAD_KEY, HEAD_KEY)], local_sem.at[4]),
        pltpu.make_async_copy(w_value, wvg.at[:, :, pl.ds(0, 128)], local_sem.at[5]),
        pltpu.make_async_copy(w_gate, wvg.at[:, :, pl.ds(128, 128)], local_sem.at[6]),
        pltpu.make_async_copy(out_gain, ogain_v, local_sem.at[7]),
        pltpu.make_async_copy(w_out, wout_v, local_sem.at[8]),
        pltpu.make_async_copy(decay_offset, off_v, local_sem.at[9]),
    ]
    for f in fetches:
        f.start()
    state_in = [
        pltpu.make_async_copy(state.at[l, :, 0], st.at[l], state_sem.at[l]) for l in range(LAYERS)
    ]
    for f in state_in:
        f.start()

    xs[...] = jnp.zeros_like(xs)
    wqkd[:, 3 * HEAD_KEY :, :] = jnp.zeros_like(wqkd[:, 3 * HEAD_KEY :, :])

    fetches[0].wait()
    first = h_v[...].astype(jnp.float32)
    pk[0, 0:1, 0:feats] = first[0:1]
    pk[0, 0:1, feats : feats + half] = first[1:2, 0:half]
    pk[0, 1:2, 0:half] = first[1:2, half:feats]
    pk[0, 1:2, half : half + feats] = first[2:3]
    ag[0, p] = pk[0].astype(jnp.bfloat16)

    with jax.named_scope("barrier"):
        pl.semaphore_wait(barrier, len(greeted))

    def offset(i):
        k = (i + 1) // 2
        return jnp.where(i % 2 == 1, n_dp - k, k)

    def source_group(i):
        return (group + offset(i)) % n_dp

    def row_group(l, i):
        return (source_group(i) + l * (n_dp // 2)) % n_dp

    def source(i):
        return source_group(i) * members + place

    def remote(src, dst, send_sem, recv_sem, device):
        return pltpu.make_async_remote_copy(
            src_ref=src,
            dst_ref=dst,
            send_sem=send_sem,
            recv_sem=recv_sem,
            device_id=device,
            device_id_type=MESH,
        )

    def arrived(ref, sem):
        remote(ref, ref, far_send_sem.at[0], sem, {"tp": anti}).wait_recv()

    def far_copy(l, sigma, i, to):
        return remote(
            ag.at[l, sigma], ag.at[l, sigma], far_send_sem.at[l], far_sem.at[l, i], {"tp": to}
        )

    def up(k):
        return (p + members * k) % n_tp

    def down(k):
        return (p - members * k + n_tp) % n_tp

    def to_mates(l, i):
        sigma = source(i)
        for j in range(members - 1):
            remote(
                ag.at[l, sigma],
                ag.at[l, sigma],
                mate_send_sem.at[l],
                mate_sem.at[l, i],
                {"tp": mate(j)},
            ).start()

    def begin(l):
        if l == 0:
            far_copy(l, p, 1, up(1)).start()
            far_copy(l, p, 2, down(1)).start()
        else:
            for k in range(n_dp // 2, 0, -1):
                far_copy(l, p, 2 * k - 1, up(k)).start()
                if 2 * k < n_dp:
                    far_copy(l, p, 2 * k, down(k)).start()
        to_mates(l, 0)

    def forward(l, i):
        sigma = source(i)
        arrived(ag.at[l, sigma], far_sem.at[l, i])
        if l == 0 and i + 2 < n_dp:
            far_copy(l, sigma, i + 2, up(1) if i % 2 == 1 else down(1)).start()

        to_mates(l, i)

    lane = lax.broadcasted_iota(jnp.int32, (seqs, 512), 1)

    def project(l, i):
        sg = source_group(i)
        arrived(ag.at[l, pl.ds(0, members - 1)], mate_sem.at[l, i])
        for j in range(members):
            b = ag[l, sg * members + j].astype(jnp.float32)
            xs[3 * j : 3 * j + 1, :] = b[0:1, 0:feats]
            xs[3 * j + 1 : 3 * j + 2, 0:half] = b[0:1, feats : feats + half]
            xs[3 * j + 1 : 3 * j + 2, half:feats] = b[1:2, 0:half]
            xs[3 * j + 2 : 3 * j + 3, :] = b[1:2, half : half + feats]
        x = xs[...]
        squares = jnp.sum(x * x, axis=1, keepdims=True)[0:seqs]
        scaled = (x * gain_v[l : l + 1, :]).astype(jnp.bfloat16)
        y = jnp.concatenate(
            [
                lax.dot_general(
                    scaled,
                    wqkd[l],
                    (((1,), (1,)), ((), ())),
                    preferred_element_type=jnp.float32,
                ),
                jnp.dot(scaled, wvg[l], preferred_element_type=jnp.float32),
            ],
            axis=1,
        )[0:seqs]
        high = squares.astype(jnp.bfloat16).astype(jnp.float32)
        rest = squares - high
        mid = rest.astype(jnp.bfloat16).astype(jnp.float32)
        low = rest - mid
        y = jnp.where(lane == 192, high, y)
        y = jnp.where(lane == 193, mid, y)
        y = jnp.where(lane == 194, low, y)
        part_send[l, i] = y.astype(jnp.bfloat16)
        to = row_group(l, i)

        @pl.when(to != d)
        def _():
            slot = (d - to + n_dp) % n_dp - 1
            remote(
                part_send.at[l, i],
                part_recv.at[l, slot],
                part_send_sem.at[l],
                part_sem.at[l],
                {"dp": to},
            ).start()

    def gat_copy(l, i, peer):
        return remote(
            gat.at[l, i], gat.at[l, i], gat_send_sem.at[l], gat_sem.at[l, i], {"dp": peer}
        )

    def update(l, i):
        arrived(part_recv.at[l], part_sem.at[l])
        total = part_send[l, i].astype(jnp.float32)
        for k in range(n_dp - 1):
            total += part_recv[l, k].astype(jnp.float32)
        squares = jnp.sum(total[:, 192:195], axis=1, keepdims=True)
        projected = total * lax.rsqrt(squares / D + epsilon)
        query_key = projected[:, 0:128]
        decay_pre = projected[:, 128:256]
        value = projected[:, 256:384]
        gate = projected[:, 384:512]
        log_sig = jnp.minimum(decay_pre, 0.0) - jnp.log1p(jnp.exp(-jnp.abs(decay_pre)))
        rate = jnp.exp(log_sig[:, 0:HEAD_KEY] / softness_factor + off_v[:, l, :])
        columns_qk = jnp.transpose(query_key, (1, 0))
        columns_rate = jnp.transpose(jnp.concatenate([rate, rate], axis=1), (1, 0))
        outs = []
        for s in range(seqs):
            q = columns_qk[0:HEAD_KEY, s : s + 1]
            k = columns_qk[HEAD_KEY : 2 * HEAD_KEY, s : s + 1] * HEAD_KEY ** (-0.5)
            r = columns_rate[0:HEAD_KEY, s : s + 1]
            fresh = r * st[l, s] + k * value[s : s + 1, :]
            new_state[l, s, 0] = fresh
            outs.append(jnp.sum(q * fresh, axis=0, keepdims=True))
        readout = jnp.concatenate(outs, axis=0)
        normed = readout * lax.rsqrt(jnp.mean(readout * readout, axis=1, keepdims=True) + epsilon)
        normed = normed * ogain_v[l : l + 1, :]
        silu = gate / (1.0 + jnp.exp(-gate))
        gat[l, i] = (normed * silu).astype(jnp.bfloat16)
        for j in range(n_dp - 1):
            gat_copy(l, i, (d + 1 + j) % n_dp).start()

    def out_project(l, i):
        @pl.when(row_group(l, i) != d)
        def _():
            arrived(gat.at[l, i], gat_sem.at[l, i])

        y = jnp.dot(gat[l, i], wout_v[l], preferred_element_type=jnp.float32)
        for j in range(members):
            pk[j, 0:1, 0:feats] = y[3 * j : 3 * j + 1]
            pk[j, 0:1, feats : feats + half] = y[3 * j + 1 : 3 * j + 2, 0:half]
            pk[j, 1:2, 0:half] = y[3 * j + 1 : 3 * j + 2, half:feats]
            pk[j, 1:2, half : half + feats] = y[3 * j + 2 : 3 * j + 3]
        for j in range(members):
            terms[l, members * i + j] = pk[j].astype(jnp.bfloat16)
        base = source_group(i) * members + n_tp // 2
        for j in range(members):
            owner = (base + j) % n_tp

            @pl.when(owner != p)
            def _():
                remote(
                    terms.at[l, members * i + j],
                    terms_in.at[l, (p - owner + n_tp) % n_tp - 1],
                    terms_send_sem.at[l],
                    terms_sem.at[l],
                    {"tp": owner},
                ).start()

    def nearby(k):
        return [i for i in (2 * k - 1, 2 * k) if 0 <= i < n_dp]

    def mine(l, k):
        wanted = [row_group(l, i) == d for i in nearby(k)]

        @pl.when(functools.reduce(jnp.logical_or, wanted))
        def _():
            update(l, jnp.where(wanted[0], nearby(k)[0], nearby(k)[-1]))

    for l in range(LAYERS):
        begin(l)
        if l == 0:
            for f in fetches[1:]:
                f.wait()
        state_in[l].wait()
        for step in STEPS[l]:
            k = int(step[1:])
            if step[0] == "U":
                mine(l, k)
            else:
                fn = {"F": forward, "A": project, "O": out_project}[step[0]]
                for i in nearby(k):
                    fn(l, i)

        with jax.named_scope("owner_wait"):
            arrived(terms_in.at[l], terms_sem.at[l])
        total = terms[l, members * last + place].astype(jnp.float32)
        total += jnp.sum(terms_in[l].astype(jnp.float32), axis=0)
        result = (total + ag[l, anti].astype(jnp.float32)).astype(jnp.bfloat16)
        if l + 1 < LAYERS:
            ag[l + 1, p] = result
        else:
            b = result.astype(jnp.float32)
            xs[0:1, :] = b[0:1, 0:feats]
            xs[1:2, 0:half] = b[0:1, feats : feats + half]
            xs[1:2, half:feats] = b[1:2, 0:half]
            xs[2:3, :] = b[1:2, half : half + feats]
            hidden_out[...] = xs[0:rows, :].astype(jnp.bfloat16)

    for l in range(LAYERS):
        many = (members - 1) * n_dp
        for ref, sem in (
            (ag.at[l, pl.ds(0, n_dp - 1)], far_send_sem),
            (ag.at[l, pl.ds(0, many)], mate_send_sem),
            (terms_in.at[l], terms_send_sem),
            (part_recv.at[l], part_send_sem),
            (gat.at[l, pl.ds(0, n_dp - 1)], gat_send_sem),
        ):
            remote(ref, ref, sem.at[l], part_sem.at[l], {"tp": anti}).wait_send()


def store_results(h, s, h_out, s_out, sem):
    copies = [
        pltpu.make_async_copy(s, s_out, sem.at[0]),
        pltpu.make_async_copy(h, h_out, sem.at[1]),
    ]
    for c in copies:
        c.start()
    for c in copies:
        c.wait()


def per_device(n_tp, n_dp, *args):
    hidden, state = args[0], args[10]
    rows, feats = hidden.shape
    members = n_tp // n_dp
    seqs = state.shape[1]
    block = (2, rows * feats // 2)
    hbm_spec = pl.BlockSpec(memory_space=pltpu.HBM)
    vmem_spec = pl.BlockSpec(memory_space=pltpu.VMEM)
    args = list(args)
    for i in (2, 3, 4):
        args[i] = jnp.swapaxes(args[i], 1, 2)
    args[9] = jnp.swapaxes(args[9], 0, 1)
    bf16, f32 = jnp.bfloat16, jnp.float32
    cols = 512
    dma = pltpu.SemaphoreType.DMA
    results = pl.pallas_call(
        functools.partial(kernel, n_tp, n_dp),
        name="decode",
        out_shape=(
            pltpu.VMEM(hidden.shape, hidden.dtype),
            pltpu.VMEM(state.shape, state.dtype),
        ),
        in_specs=[hbm_spec] * 11,
        out_specs=(vmem_spec, vmem_spec),
        scratch_shapes=[
            pltpu.VMEM(hidden.shape, bf16),
            pltpu.VMEM(args[1].shape, f32),
            pltpu.VMEM((LAYERS, 4 * HEAD_KEY, feats), bf16),
            pltpu.VMEM((LAYERS, feats, 2 * VALUE_CHANNELS), bf16),
            pltpu.VMEM(args[7].shape, f32),
            pltpu.VMEM(args[8].shape, bf16),
            pltpu.VMEM(args[9].shape, f32),
            pltpu.VMEM((LAYERS, seqs) + state.shape[3:], f32),
            pltpu.VMEM((LAYERS, n_tp) + block, bf16),
            pltpu.VMEM((LAYERS, n_dp, seqs, cols), bf16),
            pltpu.VMEM((LAYERS, n_dp - 1, seqs, cols), bf16),
            pltpu.VMEM((LAYERS, n_dp, seqs, VALUE_CHANNELS), bf16),
            pltpu.VMEM((LAYERS, n_tp) + block, bf16),
            pltpu.VMEM((LAYERS, n_tp - 1) + block, bf16),
            pltpu.VMEM((16, feats), f32),
            pltpu.VMEM((members,) + block, f32),
            dma((10,)),
            dma((LAYERS,)),
            dma((LAYERS,)),
            dma((LAYERS, n_dp)),
            dma((LAYERS,)),
            dma((LAYERS, n_dp)),
            dma((LAYERS,)),
            dma((LAYERS,)),
            dma((LAYERS,)),
            dma((LAYERS, n_dp)),
            dma((LAYERS,)),
            dma((LAYERS,)),
        ],
        compiler_params=pltpu.CompilerParams(
            collective_id=0, has_side_effects=True, vmem_limit_bytes=64000000
        ),
    )(*args)
    return pl.pallas_call(
        store_results,
        name="store_results",
        out_shape=tuple(jax.ShapeDtypeStruct(r.shape, r.dtype) for r in (hidden, state)),
        in_specs=[vmem_spec] * 2,
        out_specs=(hbm_spec, hbm_spec),
        scratch_shapes=[dma((2,))],
    )(*[pltpu.with_memory_space_constraint(r, pltpu.VMEM) for r in results])


def solution(mesh):
    return jax.shard_map(
        functools.partial(per_device, mesh.shape["tp"], mesh.shape["dp"]),
        mesh=mesh,
        in_specs=(
            P(("grp", "tp"), "dp"),
            P(None, "dp"),
            P(None, "dp", "tp"),
            P(None, "dp", "tp"),
            P(None, "dp", "tp"),
            P(None, "dp", "tp"),
            P(None, "dp", "tp"),
            P(None, "tp"),
            P(None, "tp", "dp"),
            P(None, ("grp", "dp"), "tp"),
            P(None, ("grp", "dp"), "tp", None, None),
        ),
        out_specs=(P(("grp", "tp"), "dp"), P(None, ("grp", "dp"), "tp", None, None)),
        check_vma=False,
    )
```

```python
import functools

import jax
import jax.numpy as jnp
from jax import lax
from jax.experimental import pallas as pl
from jax.experimental.pallas import tpu as pltpu
from jax.sharding import PartitionSpec as P

D = 4096
HEAD_KEY = 64
VALUE_CHANNELS = 128
LAYERS = 2

epsilon = 1e-06
softness_factor = 16.0

MESH = pl.DeviceIdType.MESH

STEPS = (
    (
        "A0", "F1", "F2", "A1", "U0", "F3", "A2", "U1",
        "F4", "O0", "A3", "U2", "O1", "A4", "U3", "O2",
        "U4", "O3", "O4",
    ),
    (
        "A0", "F1", "F2", "U0", "A1", "F3", "A2", "U1",
        "F4", "A3", "O0", "U2", "O1", "A4", "U3", "O2",
        "U4", "O3", "O4",
    ),
)


def kernel(
    n_tp,
    n_dp,
    hidden,
    gain,
    w_query,
    w_key,
    w_decay,
    w_value,
    w_gate,
    out_gain,
    w_out,
    decay_offset,
    state,
    hidden_out,
    new_state,
    h_v,
    gain_v,
    wqkd,
    wvg,
    ogain_v,
    wout_v,
    off_v,
    st,
    ag,
    part_send,
    part_recv,
    gat,
    terms,
    terms_in,
    xs,
    pk,
    local_sem,
    state_sem,
    ready,
    all_send_sem,
    far_send_sem,
    far_sem,
    mate_send_sem,
    mate_sem,
    part_send_sem,
    part_sem,
    gat_send_sem,
    gat_sem,
    terms_send_sem,
    terms_sem,
):
    rows, feats = h_v.shape
    half = feats // 2
    members = n_tp // n_dp
    seqs = rows * members
    p = lax.axis_index("tp")
    d = lax.axis_index("dp")
    group = p // members
    place = p % members
    anti = (p + n_tp // 2) % n_tp
    last = n_dp - 1

    def mate(j):
        return group * members + (place + 1 + j) % members

    def up(k):
        return (p + members * k) % n_tp

    def down(k):
        return (p - members * k + n_tp) % n_tp

    quads = [up(k) for k in range(1, n_dp // 2 + 1)] + [down(k) for k in range(1, n_dp // 2)]
    barrier = pltpu.get_barrier_semaphore()

    def greet(device):
        pl.semaphore_signal(barrier, inc=1, device_id=device, device_id_type=MESH)

    for j in range(members - 1):
        greet({"tp": mate(j)})
    for peer in quads:

        @pl.when((peer > p) | (peer == p - members))
        def _():
            greet({"tp": peer})

    for j in range(n_dp - 1):
        greet({"dp": (d + 1 + j) % n_dp})
    heard = members - 1 + n_dp - 1
    for peer in quads:
        heard += jnp.where((peer < p) | (peer == p + members), 1, 0)

    fetches = [
        pltpu.make_async_copy(hidden, h_v, local_sem.at[0]),
        pltpu.make_async_copy(gain, gain_v, local_sem.at[1]),
        pltpu.make_async_copy(w_query, wqkd.at[:, pl.ds(0, HEAD_KEY)], local_sem.at[2]),
        pltpu.make_async_copy(w_key, wqkd.at[:, pl.ds(HEAD_KEY, HEAD_KEY)], local_sem.at[3]),
        pltpu.make_async_copy(w_decay, wqkd.at[:, pl.ds(2 * HEAD_KEY, HEAD_KEY)], local_sem.at[4]),
        pltpu.make_async_copy(w_value, wvg.at[:, :, pl.ds(0, 128)], local_sem.at[5]),
        pltpu.make_async_copy(w_gate, wvg.at[:, :, pl.ds(128, 128)], local_sem.at[6]),
        pltpu.make_async_copy(out_gain, ogain_v, local_sem.at[7]),
        pltpu.make_async_copy(w_out, wout_v, local_sem.at[8]),
        pltpu.make_async_copy(decay_offset, off_v, local_sem.at[9]),
    ]
    for f in fetches:
        f.start()
    state_in = [
        pltpu.make_async_copy(state.at[l, :, 0], st.at[l], state_sem.at[l]) for l in range(LAYERS)
    ]
    for f in state_in:
        f.start()

    xs[...] = jnp.zeros_like(xs)
    wqkd[:, 3 * HEAD_KEY :, :] = jnp.zeros_like(wqkd[:, 3 * HEAD_KEY :, :])

    fetches[0].wait()
    first = h_v[...].astype(jnp.float32)
    pk[0, 0:1, 0:feats] = first[0:1]
    pk[0, 0:1, feats : feats + half] = first[1:2, 0:half]
    pk[0, 1:2, 0:half] = first[1:2, half:feats]
    pk[0, 1:2, half : half + feats] = first[2:3]
    ag[0, p] = pk[0].astype(jnp.bfloat16)

    with jax.named_scope("barrier"):
        pl.semaphore_wait(barrier, heard)

    @pl.when(up(1) < p)
    def _():
        pl.semaphore_signal(ready, inc=1, device_id={"tp": up(1)}, device_id_type=MESH)

    def offset(i):
        k = (i + 1) // 2
        return jnp.where(i % 2 == 1, n_dp - k, k)

    def source_group(i):
        return (group + offset(i)) % n_dp

    def row_group(l, i):
        return (source_group(i) + l * (n_dp // 2)) % n_dp

    def source(i):
        return source_group(i) * members + place

    def remote(src, dst, send_sem, recv_sem, device):
        return pltpu.make_async_remote_copy(
            src_ref=src,
            dst_ref=dst,
            send_sem=send_sem,
            recv_sem=recv_sem,
            device_id=device,
            device_id_type=MESH,
        )

    def arrived(ref, sem):
        remote(ref, ref, all_send_sem, sem, {"tp": anti}).wait_recv()

    def far_copy(sigma, i, to, relayed):
        return remote(
            ag.at[0, sigma], ag.at[0, sigma], far_send_sem.at[relayed, i], far_sem.at[0, i], {"tp": to}
        )

    def own_rows(act):
        for k in range(n_dp // 2, 0, -1):
            for i, to in ((2 * k - 1, up(k)), (2 * k, down(k))):
                if i == n_dp:
                    continue

                @pl.when((to < p) | (to == p + members))
                def _():
                    act(far_copy(p, i, to, 0))

    def across(act):
        @pl.when(down(1) > p)
        def _():
            act(far_copy(p, 2, down(1), 0))

    def relay(i, act):
        sigma = source(i)
        to = up(1) if i % 2 == 1 else down(1)

        @pl.when(to > sigma)
        def _():
            act(far_copy(sigma, i + 2, to, 1))

    def to_mates(l, i):
        sigma = source(i)
        for j in range(members - 1):
            remote(
                ag.at[l, sigma],
                ag.at[l, sigma],
                mate_send_sem.at[l],
                mate_sem.at[l, i],
                {"tp": mate(j)},
            ).start()

    def begin(l):
        if l == 0:
            own_rows(lambda copy: copy.start())
            to_mates(l, 0)

            @pl.when(down(1) > p)
            def _():
                pl.semaphore_wait(ready, 1)

            across(lambda copy: copy.start())
        else:
            for k in range(n_dp // 2, 0, -1):
                for i, to in ((2 * k - 1, up(k)), (2 * k, down(k))):
                    if i < n_dp:
                        remote(
                            ag.at[l, p], ag.at[l, p], all_send_sem, far_sem.at[l, i], {"tp": to}
                        ).start()
            to_mates(l, 0)

    def forward(l, i):
        arrived(ag.at[l, source(i)], far_sem.at[l, i])
        if l == 0 and i + 2 < n_dp:
            relay(i, lambda copy: copy.start())
        to_mates(l, i)

    lane = lax.broadcasted_iota(jnp.int32, (seqs, 512), 1)

    def project(l, i):
        sg = source_group(i)
        arrived(ag.at[l, pl.ds(0, members - 1)], mate_sem.at[l, i])
        for j in range(members):
            b = ag[l, sg * members + j].astype(jnp.float32)
            xs[3 * j : 3 * j + 1, :] = b[0:1, 0:feats]
            xs[3 * j + 1 : 3 * j + 2, 0:half] = b[0:1, feats : feats + half]
            xs[3 * j + 1 : 3 * j + 2, half:feats] = b[1:2, 0:half]
            xs[3 * j + 2 : 3 * j + 3, :] = b[1:2, half : half + feats]
        x = xs[...]
        squares = jnp.sum(x * x, axis=1, keepdims=True)[0:seqs]
        scaled = (x * gain_v[l : l + 1, :]).astype(jnp.bfloat16)
        y = jnp.concatenate(
            [
                lax.dot_general(
                    scaled,
                    wqkd[l],
                    (((1,), (1,)), ((), ())),
                    preferred_element_type=jnp.float32,
                ),
                jnp.dot(scaled, wvg[l], preferred_element_type=jnp.float32),
            ],
            axis=1,
        )[0:seqs]
        high = squares.astype(jnp.bfloat16).astype(jnp.float32)
        rest = squares - high
        mid = rest.astype(jnp.bfloat16).astype(jnp.float32)
        low = rest - mid
        y = jnp.where(lane == 192, high, y)
        y = jnp.where(lane == 193, mid, y)
        y = jnp.where(lane == 194, low, y)
        part_send[l, i] = y.astype(jnp.bfloat16)
        to = row_group(l, i)

        @pl.when(to != d)
        def _():
            slot = (d - to + n_dp) % n_dp - 1
            remote(
                part_send.at[l, i],
                part_recv.at[l, slot],
                part_send_sem.at[l],
                part_sem.at[l],
                {"dp": to},
            ).start()

    def gat_copy(l, i, peer):
        return remote(
            gat.at[l, i], gat.at[l, i], gat_send_sem.at[l], gat_sem.at[l, i], {"dp": peer}
        )

    def update(l, i):
        arrived(part_recv.at[l], part_sem.at[l])
        total = part_send[l, i].astype(jnp.float32)
        for k in range(n_dp - 1):
            total += part_recv[l, k].astype(jnp.float32)
        squares = jnp.sum(total[:, 192:195], axis=1, keepdims=True)
        projected = total * lax.rsqrt(squares / D + epsilon)
        query_key = projected[:, 0:128]
        decay_pre = projected[:, 128:256]
        value = projected[:, 256:384]
        gate = projected[:, 384:512]
        log_sig = jnp.minimum(decay_pre, 0.0) - jnp.log1p(jnp.exp(-jnp.abs(decay_pre)))
        rate = jnp.exp(log_sig[:, 0:HEAD_KEY] / softness_factor + off_v[:, l, :])
        query = query_key[:, 0:HEAD_KEY]
        key = query_key[:, HEAD_KEY : 2 * HEAD_KEY] * HEAD_KEY ** (-0.5)
        columns = jnp.transpose(jnp.concatenate([query * rate, rate], axis=1), (1, 0))
        outs = []
        for s in range(seqs):
            weight = columns[0:HEAD_KEY, s : s + 1]
            outs.append(jnp.sum(weight * st[l, s], axis=0, keepdims=True))
        readout = jnp.concatenate(outs, axis=0)
        readout += jnp.sum(query * key, axis=1, keepdims=True) * value
        normed = readout * lax.rsqrt(jnp.mean(readout * readout, axis=1, keepdims=True) + epsilon)
        normed = normed * ogain_v[l : l + 1, :]
        silu = gate / (1.0 + jnp.exp(-gate))
        gat[l, i] = (normed * silu).astype(jnp.bfloat16)
        for j in range(n_dp - 1):
            gat_copy(l, i, (d + 1 + j) % n_dp).start()
        columns_key = jnp.transpose(jnp.concatenate([key, key], axis=1), (1, 0))
        for s in range(seqs):
            r = columns[HEAD_KEY : 2 * HEAD_KEY, s : s + 1]
            k = columns_key[0:HEAD_KEY, s : s + 1]
            new_state[l, s, 0] = r * st[l, s] + k * value[s : s + 1, :]

    def out_project(l, i):
        @pl.when(row_group(l, i) != d)
        def _():
            arrived(gat.at[l, i], gat_sem.at[l, i])

        y = jnp.dot(gat[l, i], wout_v[l], preferred_element_type=jnp.float32)
        for j in range(members):
            pk[j, 0:1, 0:feats] = y[3 * j : 3 * j + 1]
            pk[j, 0:1, feats : feats + half] = y[3 * j + 1 : 3 * j + 2, 0:half]
            pk[j, 1:2, 0:half] = y[3 * j + 1 : 3 * j + 2, half:feats]
            pk[j, 1:2, half : half + feats] = y[3 * j + 2 : 3 * j + 3]
        for j in range(members):
            terms[l, members * i + j] = pk[j].astype(jnp.bfloat16)
        base = source_group(i) * members + n_tp // 2
        for j in range(members):
            owner = (base + j) % n_tp

            @pl.when(owner != p)
            def _():
                remote(
                    terms.at[l, members * i + j],
                    terms_in.at[l, (p - owner + n_tp) % n_tp - 1],
                    terms_send_sem.at[l],
                    terms_sem.at[l],
                    {"tp": owner},
                ).start()

    def nearby(k):
        return [i for i in (2 * k - 1, 2 * k) if 0 <= i < n_dp]

    def mine(l, k):
        wanted = [row_group(l, i) == d for i in nearby(k)]

        @pl.when(functools.reduce(jnp.logical_or, wanted))
        def _():
            update(l, jnp.where(wanted[0], nearby(k)[0], nearby(k)[-1]))

    for l in range(LAYERS):
        begin(l)
        if l == 0:
            for f in fetches[1:]:
                f.wait()
        state_in[l].wait()
        for step in STEPS[l]:
            k = int(step[1:])
            if step[0] == "U":
                mine(l, k)
            else:
                fn = {"F": forward, "A": project, "O": out_project}[step[0]]
                for i in nearby(k):
                    fn(l, i)

        with jax.named_scope("owner_wait"):
            arrived(terms_in.at[l], terms_sem.at[l])
        total = terms[l, members * last + place].astype(jnp.float32)
        total += jnp.sum(terms_in[l].astype(jnp.float32), axis=0)
        result = (total + ag[l, anti].astype(jnp.float32)).astype(jnp.bfloat16)
        if l + 1 < LAYERS:
            ag[l + 1, p] = result
        else:
            b = result.astype(jnp.float32)
            xs[0:1, :] = b[0:1, 0:feats]
            xs[1:2, 0:half] = b[0:1, feats : feats + half]
            xs[1:2, half:feats] = b[1:2, 0:half]
            xs[2:3, :] = b[1:2, half : half + feats]
            hidden_out[...] = xs[0:rows, :].astype(jnp.bfloat16)

    for l in range(LAYERS):
        for ref, sem in (
            (terms_in.at[l], terms_send_sem),
            (part_recv.at[l], part_send_sem),
            (gat.at[l, pl.ds(0, n_dp - 1)], gat_send_sem),
        ):
            remote(ref, ref, sem.at[l], part_sem.at[l], {"tp": anti}).wait_send()
    for ref, sem in (
        (ag.at[0, pl.ds(0, (members - 1) * n_dp)], mate_send_sem.at[0]),
        (ag.at[1, pl.ds(0, (members - 1) * n_dp)], mate_send_sem.at[1]),
        (ag.at[1, pl.ds(0, n_dp - 1)], all_send_sem),
    ):
        remote(ref, ref, sem, part_sem.at[0], {"tp": anti}).wait_send()
    own_rows(lambda copy: copy.wait_send())
    across(lambda copy: copy.wait_send())
    for i in range(1, n_dp - 2):
        relay(i, lambda copy: copy.wait_send())


def store_results(h, s, h_out, s_out, sem):
    copies = [
        pltpu.make_async_copy(s, s_out, sem.at[0]),
        pltpu.make_async_copy(h, h_out, sem.at[1]),
    ]
    for c in copies:
        c.start()
    for c in copies:
        c.wait()


def per_device(n_tp, n_dp, *args):
    hidden, state = args[0], args[10]
    rows, feats = hidden.shape
    members = n_tp // n_dp
    seqs = state.shape[1]
    block = (2, rows * feats // 2)
    hbm_spec = pl.BlockSpec(memory_space=pltpu.HBM)
    vmem_spec = pl.BlockSpec(memory_space=pltpu.VMEM)
    args = list(args)
    for i in (2, 3, 4):
        args[i] = jnp.swapaxes(args[i], 1, 2)
    args[9] = jnp.swapaxes(args[9], 0, 1)
    bf16, f32 = jnp.bfloat16, jnp.float32
    cols = 512
    dma = pltpu.SemaphoreType.DMA
    results = pl.pallas_call(
        functools.partial(kernel, n_tp, n_dp),
        name="decode",
        out_shape=(
            pltpu.VMEM(hidden.shape, hidden.dtype),
            pltpu.VMEM(state.shape, state.dtype),
        ),
        in_specs=[hbm_spec] * 11,
        out_specs=(vmem_spec, vmem_spec),
        scratch_shapes=[
            pltpu.VMEM(hidden.shape, bf16),
            pltpu.VMEM(args[1].shape, f32),
            pltpu.VMEM((LAYERS, 4 * HEAD_KEY, feats), bf16),
            pltpu.VMEM((LAYERS, feats, 2 * VALUE_CHANNELS), bf16),
            pltpu.VMEM(args[7].shape, f32),
            pltpu.VMEM(args[8].shape, bf16),
            pltpu.VMEM(args[9].shape, f32),
            pltpu.VMEM((LAYERS, seqs) + state.shape[3:], f32),
            pltpu.VMEM((LAYERS, n_tp) + block, bf16),
            pltpu.VMEM((LAYERS, n_dp, seqs, cols), bf16),
            pltpu.VMEM((LAYERS, n_dp - 1, seqs, cols), bf16),
            pltpu.VMEM((LAYERS, n_dp, seqs, VALUE_CHANNELS), bf16),
            pltpu.VMEM((LAYERS, n_tp) + block, bf16),
            pltpu.VMEM((LAYERS, n_tp - 1) + block, bf16),
            pltpu.VMEM((16, feats), f32),
            pltpu.VMEM((members,) + block, f32),
            dma((10,)),
            dma((LAYERS,)),
            pltpu.SemaphoreType.REGULAR,
            dma(()),
            dma((2, n_dp)),
            dma((LAYERS, n_dp)),
            dma((LAYERS,)),
            dma((LAYERS, n_dp)),
            dma((LAYERS,)),
            dma((LAYERS,)),
            dma((LAYERS,)),
            dma((LAYERS, n_dp)),
            dma((LAYERS,)),
            dma((LAYERS,)),
        ],
        compiler_params=pltpu.CompilerParams(
            collective_id=0, has_side_effects=True, vmem_limit_bytes=64000000
        ),
    )(*args)
    return pl.pallas_call(
        store_results,
        name="store_results",
        out_shape=tuple(jax.ShapeDtypeStruct(r.shape, r.dtype) for r in (hidden, state)),
        in_specs=[vmem_spec] * 2,
        out_specs=(hbm_spec, hbm_spec),
        scratch_shapes=[dma((2,))],
    )(*[pltpu.with_memory_space_constraint(r, pltpu.VMEM) for r in results])


def solution(mesh):
    return jax.shard_map(
        functools.partial(per_device, mesh.shape["tp"], mesh.shape["dp"]),
        mesh=mesh,
        in_specs=(
            P(("grp", "tp"), "dp"),
            P(None, "dp"),
            P(None, "dp", "tp"),
            P(None, "dp", "tp"),
            P(None, "dp", "tp"),
            P(None, "dp", "tp"),
            P(None, "dp", "tp"),
            P(None, "tp"),
            P(None, "tp", "dp"),
            P(None, ("grp", "dp"), "tp"),
            P(None, ("grp", "dp"), "tp", None, None),
        ),
        out_specs=(P(("grp", "tp"), "dp"), P(None, ("grp", "dp"), "tp", None, None)),
        check_vma=False,
    )
```

```python
import functools

import jax
import jax.numpy as jnp
from jax import lax
from jax.experimental import pallas as pl
from jax.experimental.pallas import tpu as pltpu
from jax.sharding import PartitionSpec as P

D = 4096
HEAD_KEY = 64
VALUE_CHANNELS = 128
LAYERS = 2

epsilon = 1e-06
softness_factor = 16.0

MESH = pl.DeviceIdType.MESH

STEPS = (
    (
        "F1", "A0", "F2", "A1", "F3", "U0", "A2", "F4",
        "U1", "A3", "O0", "U2", "O1", "A4", "U3", "O2",
        "U4", "O3", "O4",
    ),
    (
        "F1", "A0", "F2", "A1", "F3", "U0", "A2", "F4",
        "U1", "A3", "O0", "U2", "A4", "O1", "U3", "U4",
        "O2", "O3", "O4",
    ),
)


def kernel(
    n_tp,
    n_dp,
    hidden,
    gain,
    w_query,
    w_key,
    w_decay,
    w_value,
    w_gate,
    out_gain,
    w_out,
    decay_offset,
    state,
    hidden_out,
    new_state,
    h_v,
    gain_v,
    wqkd,
    wvg,
    ogain_v,
    wout_v,
    off_v,
    st,
    ag,
    part_send,
    part_recv,
    gat,
    terms,
    terms_in,
    xs,
    pk,
    local_sem,
    state_sem,
    ready,
    all_send_sem,
    far_send_sem,
    far_sem,
    mate_send_sem,
    mate_sem,
    part_send_sem,
    part_sem,
    gat_send_sem,
    gat_sem,
    terms_send_sem,
    terms_sem,
):
    rows, feats = h_v.shape
    half = feats // 2
    members = n_tp // n_dp
    seqs = rows * members
    p = lax.axis_index("tp")
    d = lax.axis_index("dp")
    group = p // members
    place = p % members
    anti = (p + n_tp // 2) % n_tp
    last = n_dp - 1

    def mate(j):
        return group * members + (place + 1 + j) % members

    def up(k):
        return (p + members * k) % n_tp

    def down(k):
        return (p - members * k + n_tp) % n_tp

    quads = [up(k) for k in range(1, n_dp // 2 + 1)] + [down(k) for k in range(1, n_dp // 2)]
    barrier = pltpu.get_barrier_semaphore()

    def greet(device):
        pl.semaphore_signal(barrier, inc=1, device_id=device, device_id_type=MESH)

    for j in range(members - 1):
        greet({"tp": mate(j)})
    for peer in quads:

        @pl.when((peer > p) | (peer == p - members))
        def _():
            greet({"tp": peer})

    for j in range(n_dp - 1):
        greet({"dp": (d + 1 + j) % n_dp})
    heard = members - 1 + n_dp - 1
    for peer in quads:
        heard += jnp.where((peer < p) | (peer == p + members), 1, 0)

    fetches = [
        pltpu.make_async_copy(hidden, h_v, local_sem.at[0]),
        pltpu.make_async_copy(gain, gain_v, local_sem.at[1]),
        pltpu.make_async_copy(w_query, wqkd.at[:, pl.ds(0, HEAD_KEY)], local_sem.at[2]),
        pltpu.make_async_copy(w_key, wqkd.at[:, pl.ds(HEAD_KEY, HEAD_KEY)], local_sem.at[3]),
        pltpu.make_async_copy(w_decay, wqkd.at[:, pl.ds(2 * HEAD_KEY, HEAD_KEY)], local_sem.at[4]),
        pltpu.make_async_copy(w_value, wvg.at[:, :, pl.ds(0, 128)], local_sem.at[5]),
        pltpu.make_async_copy(w_gate, wvg.at[:, :, pl.ds(128, 128)], local_sem.at[6]),
        pltpu.make_async_copy(out_gain, ogain_v, local_sem.at[7]),
        pltpu.make_async_copy(w_out, wout_v, local_sem.at[8]),
        pltpu.make_async_copy(decay_offset, off_v, local_sem.at[9]),
    ]
    for f in fetches:
        f.start()
    state_in = [
        pltpu.make_async_copy(state.at[l, :, 0], st.at[l], state_sem.at[l]) for l in range(LAYERS)
    ]
    for f in state_in:
        f.start()

    xs[...] = jnp.zeros_like(xs)
    wqkd[:, 3 * HEAD_KEY :, :] = jnp.zeros_like(wqkd[:, 3 * HEAD_KEY :, :])

    fetches[0].wait()
    first = h_v[...].astype(jnp.float32)
    pk[0, 0:1, 0:feats] = first[0:1]
    pk[0, 0:1, feats : feats + half] = first[1:2, 0:half]
    pk[0, 1:2, 0:half] = first[1:2, half:feats]
    pk[0, 1:2, half : half + feats] = first[2:3]
    ag[0, p] = pk[0].astype(jnp.bfloat16)

    with jax.named_scope("barrier"):
        pl.semaphore_wait(barrier, heard)

    @pl.when(up(1) < p)
    def _():
        pl.semaphore_signal(ready, inc=1, device_id={"tp": up(1)}, device_id_type=MESH)

    def offset(i):
        k = (i + 1) // 2
        return jnp.where(i % 2 == 1, n_dp - k, k)

    def source_group(i):
        return (group + offset(i)) % n_dp

    def row_group(l, i):
        return (source_group(i) + l * (n_dp // 2)) % n_dp

    def source(i):
        return source_group(i) * members + place

    def remote(src, dst, send_sem, recv_sem, device):
        return pltpu.make_async_remote_copy(
            src_ref=src,
            dst_ref=dst,
            send_sem=send_sem,
            recv_sem=recv_sem,
            device_id=device,
            device_id_type=MESH,
        )

    def arrived(ref, sem):
        remote(ref, ref, all_send_sem, sem, {"tp": anti}).wait_recv()

    def far_copy(sigma, i, to, relayed):
        return remote(
            ag.at[0, sigma], ag.at[0, sigma], far_send_sem.at[relayed, i], far_sem.at[0, i], {"tp": to}
        )

    def own_rows(act):
        for k in range(n_dp // 2, 0, -1):
            for i, to in ((2 * k - 1, up(k)), (2 * k, down(k))):
                if i == n_dp:
                    continue

                @pl.when((to < p) | (to == p + members))
                def _():
                    act(far_copy(p, i, to, 0))

    def across(act):
        @pl.when(down(1) > p)
        def _():
            act(far_copy(p, 2, down(1), 0))

    def relay(i, act):
        sigma = source(i)
        to = up(1) if i % 2 == 1 else down(1)

        @pl.when(to > sigma)
        def _():
            act(far_copy(sigma, i + 2, to, 1))

    def to_mates(l, i):
        sigma = source(i)
        for j in range(members - 1):
            remote(
                ag.at[l, sigma],
                ag.at[l, sigma],
                mate_send_sem.at[l],
                mate_sem.at[l, i],
                {"tp": mate(j)},
            ).start()

    def begin(l):
        if l == 0:
            own_rows(lambda copy: copy.start())
            to_mates(l, 0)

            @pl.when(down(1) > p)
            def _():
                pl.semaphore_wait(ready, 1)

            across(lambda copy: copy.start())
        else:
            for k in range(n_dp // 2, 0, -1):
                for i, to in ((2 * k - 1, up(k)), (2 * k, down(k))):
                    if i < n_dp:
                        remote(
                            ag.at[l, p], ag.at[l, p], all_send_sem, far_sem.at[l, i], {"tp": to}
                        ).start()
            to_mates(l, 0)

    def forward(l, i):
        arrived(ag.at[l, source(i)], far_sem.at[l, i])
        if l == 0 and i + 2 < n_dp:
            relay(i, lambda copy: copy.start())
        to_mates(l, i)

    lane = lax.broadcasted_iota(jnp.int32, (seqs, 512), 1)

    def project(l, i):
        sg = source_group(i)
        arrived(ag.at[l, pl.ds(0, members - 1)], mate_sem.at[l, i])
        for j in range(members):
            b = ag[l, sg * members + j].astype(jnp.float32)
            xs[3 * j : 3 * j + 1, :] = b[0:1, 0:feats]
            xs[3 * j + 1 : 3 * j + 2, 0:half] = b[0:1, feats : feats + half]
            xs[3 * j + 1 : 3 * j + 2, half:feats] = b[1:2, 0:half]
            xs[3 * j + 2 : 3 * j + 3, :] = b[1:2, half : half + feats]
        x = xs[...]
        squares = jnp.sum(x * x, axis=1, keepdims=True)[0:seqs]
        scaled = (x * gain_v[l : l + 1, :]).astype(jnp.bfloat16)
        y = jnp.concatenate(
            [
                lax.dot_general(
                    scaled,
                    wqkd[l],
                    (((1,), (1,)), ((), ())),
                    preferred_element_type=jnp.float32,
                ),
                jnp.dot(scaled, wvg[l], preferred_element_type=jnp.float32),
            ],
            axis=1,
        )[0:seqs]
        high = squares.astype(jnp.bfloat16).astype(jnp.float32)
        rest = squares - high
        mid = rest.astype(jnp.bfloat16).astype(jnp.float32)
        low = rest - mid
        y = jnp.where(lane == 192, high, y)
        y = jnp.where(lane == 193, mid, y)
        y = jnp.where(lane == 194, low, y)
        part_send[l, i] = y.astype(jnp.bfloat16)
        to = row_group(l, i)

        @pl.when(to != d)
        def _():
            slot = (d - to + n_dp) % n_dp - 1
            remote(
                part_send.at[l, i],
                part_recv.at[l, slot],
                part_send_sem.at[l],
                part_sem.at[l],
                {"dp": to},
            ).start()

    def gat_copy(l, i, peer):
        return remote(
            gat.at[l, i], gat.at[l, i], gat_send_sem.at[l], gat_sem.at[l, i], {"dp": peer}
        )

    def update(l, i):
        arrived(part_recv.at[l], part_sem.at[l])
        total = part_send[l, i].astype(jnp.float32)
        for k in range(n_dp - 1):
            total += part_recv[l, k].astype(jnp.float32)
        squares = jnp.sum(total[:, 192:195], axis=1, keepdims=True)
        projected = total * lax.rsqrt(squares / D + epsilon)
        query_key = projected[:, 0:128]
        decay_pre = projected[:, 128:256]
        value = projected[:, 256:384]
        gate = projected[:, 384:512]
        log_sig = jnp.minimum(decay_pre, 0.0) - jnp.log1p(jnp.exp(-jnp.abs(decay_pre)))
        rate = jnp.exp(log_sig[:, 0:HEAD_KEY] / softness_factor + off_v[:, l, :])
        query = query_key[:, 0:HEAD_KEY]
        key = query_key[:, HEAD_KEY : 2 * HEAD_KEY] * HEAD_KEY ** (-0.5)
        columns = jnp.transpose(jnp.concatenate([query * rate, rate], axis=1), (1, 0))
        outs = []
        for s in range(seqs):
            weight = columns[0:HEAD_KEY, s : s + 1]
            outs.append(jnp.sum(weight * st[l, s], axis=0, keepdims=True))
        readout = jnp.concatenate(outs, axis=0)
        readout += jnp.sum(query * key, axis=1, keepdims=True) * value
        normed = readout * lax.rsqrt(jnp.mean(readout * readout, axis=1, keepdims=True) + epsilon)
        normed = normed * ogain_v[l : l + 1, :]
        silu = gate / (1.0 + jnp.exp(-gate))
        gat[l, i] = (normed * silu).astype(jnp.bfloat16)
        for j in range(n_dp - 1):
            gat_copy(l, i, (d + 1 + j) % n_dp).start()
        columns_key = jnp.transpose(jnp.concatenate([key, key], axis=1), (1, 0))
        for s in range(seqs):
            r = columns[HEAD_KEY : 2 * HEAD_KEY, s : s + 1]
            k = columns_key[0:HEAD_KEY, s : s + 1]
            new_state[l, s, 0] = r * st[l, s] + k * value[s : s + 1, :]

    def out_project(l, i):
        @pl.when(row_group(l, i) != d)
        def _():
            arrived(gat.at[l, i], gat_sem.at[l, i])

        y = jnp.dot(gat[l, i], wout_v[l], preferred_element_type=jnp.float32)
        for j in range(members):
            pk[j, 0:1, 0:feats] = y[3 * j : 3 * j + 1]
            pk[j, 0:1, feats : feats + half] = y[3 * j + 1 : 3 * j + 2, 0:half]
            pk[j, 1:2, 0:half] = y[3 * j + 1 : 3 * j + 2, half:feats]
            pk[j, 1:2, half : half + feats] = y[3 * j + 2 : 3 * j + 3]
        for j in range(members):
            terms[l, members * i + j] = pk[j].astype(jnp.bfloat16)
        base = source_group(i) * members + n_tp // 2
        for j in range(members):
            owner = (base + j) % n_tp

            @pl.when(owner != p)
            def _():
                remote(
                    terms.at[l, members * i + j],
                    terms_in.at[l, (p - owner + n_tp) % n_tp - 1],
                    terms_send_sem.at[l],
                    terms_sem.at[l],
                    {"tp": owner},
                ).start()

    def nearby(k):
        return [i for i in (2 * k - 1, 2 * k) if 0 <= i < n_dp]

    def mine(l, k):
        wanted = [row_group(l, i) == d for i in nearby(k)]

        @pl.when(functools.reduce(jnp.logical_or, wanted))
        def _():
            update(l, jnp.where(wanted[0], nearby(k)[0], nearby(k)[-1]))

    for l in range(LAYERS):
        begin(l)
        if l == 0:
            for f in fetches[1:]:
                f.wait()
        state_in[l].wait()
        for step in STEPS[l]:
            k = int(step[1:])
            if step[0] == "U":
                mine(l, k)
            else:
                fn = {"F": forward, "A": project, "O": out_project}[step[0]]
                for i in nearby(k):
                    fn(l, i)

        with jax.named_scope("owner_wait"):
            arrived(terms_in.at[l], terms_sem.at[l])
        total = terms[l, members * last + place].astype(jnp.float32)
        total += jnp.sum(terms_in[l].astype(jnp.float32), axis=0)
        result = (total + ag[l, anti].astype(jnp.float32)).astype(jnp.bfloat16)
        if l + 1 < LAYERS:
            ag[l + 1, p] = result
        else:
            b = result.astype(jnp.float32)
            xs[0:1, :] = b[0:1, 0:feats]
            xs[1:2, 0:half] = b[0:1, feats : feats + half]
            xs[1:2, half:feats] = b[1:2, 0:half]
            xs[2:3, :] = b[1:2, half : half + feats]
            hidden_out[...] = xs[0:rows, :].astype(jnp.bfloat16)

    for l in range(LAYERS):
        for ref, sem in (
            (terms_in.at[l], terms_send_sem),
            (part_recv.at[l], part_send_sem),
            (gat.at[l, pl.ds(0, n_dp - 1)], gat_send_sem),
        ):
            remote(ref, ref, sem.at[l], part_sem.at[l], {"tp": anti}).wait_send()
    for ref, sem in (
        (ag.at[0, pl.ds(0, (members - 1) * n_dp)], mate_send_sem.at[0]),
        (ag.at[1, pl.ds(0, (members - 1) * n_dp)], mate_send_sem.at[1]),
        (ag.at[1, pl.ds(0, n_dp - 1)], all_send_sem),
    ):
        remote(ref, ref, sem, part_sem.at[0], {"tp": anti}).wait_send()
    own_rows(lambda copy: copy.wait_send())
    across(lambda copy: copy.wait_send())
    for i in range(1, n_dp - 2):
        relay(i, lambda copy: copy.wait_send())


def store_results(h, s, h_out, s_out, sem):
    copies = [
        pltpu.make_async_copy(s, s_out, sem.at[0]),
        pltpu.make_async_copy(h, h_out, sem.at[1]),
    ]
    for c in copies:
        c.start()
    for c in copies:
        c.wait()


def per_device(n_tp, n_dp, *args):
    hidden, state = args[0], args[10]
    rows, feats = hidden.shape
    members = n_tp // n_dp
    seqs = state.shape[1]
    block = (2, rows * feats // 2)
    hbm_spec = pl.BlockSpec(memory_space=pltpu.HBM)
    vmem_spec = pl.BlockSpec(memory_space=pltpu.VMEM)
    args = list(args)
    for i in (2, 3, 4):
        args[i] = jnp.swapaxes(args[i], 1, 2)
    args[9] = jnp.swapaxes(args[9], 0, 1)
    bf16, f32 = jnp.bfloat16, jnp.float32
    cols = 512
    dma = pltpu.SemaphoreType.DMA
    results = pl.pallas_call(
        functools.partial(kernel, n_tp, n_dp),
        name="decode",
        out_shape=(
            pltpu.VMEM(hidden.shape, hidden.dtype),
            pltpu.VMEM(state.shape, state.dtype),
        ),
        in_specs=[hbm_spec] * 11,
        out_specs=(vmem_spec, vmem_spec),
        scratch_shapes=[
            pltpu.VMEM(hidden.shape, bf16),
            pltpu.VMEM(args[1].shape, f32),
            pltpu.VMEM((LAYERS, 4 * HEAD_KEY, feats), bf16),
            pltpu.VMEM((LAYERS, feats, 2 * VALUE_CHANNELS), bf16),
            pltpu.VMEM(args[7].shape, f32),
            pltpu.VMEM(args[8].shape, bf16),
            pltpu.VMEM(args[9].shape, f32),
            pltpu.VMEM((LAYERS, seqs) + state.shape[3:], f32),
            pltpu.VMEM((LAYERS, n_tp) + block, bf16),
            pltpu.VMEM((LAYERS, n_dp, seqs, cols), bf16),
            pltpu.VMEM((LAYERS, n_dp - 1, seqs, cols), bf16),
            pltpu.VMEM((LAYERS, n_dp, seqs, VALUE_CHANNELS), bf16),
            pltpu.VMEM((LAYERS, n_tp) + block, bf16),
            pltpu.VMEM((LAYERS, n_tp - 1) + block, bf16),
            pltpu.VMEM((16, feats), f32),
            pltpu.VMEM((members,) + block, f32),
            dma((10,)),
            dma((LAYERS,)),
            pltpu.SemaphoreType.REGULAR,
            dma(()),
            dma((2, n_dp)),
            dma((LAYERS, n_dp)),
            dma((LAYERS,)),
            dma((LAYERS, n_dp)),
            dma((LAYERS,)),
            dma((LAYERS,)),
            dma((LAYERS,)),
            dma((LAYERS, n_dp)),
            dma((LAYERS,)),
            dma((LAYERS,)),
        ],
        compiler_params=pltpu.CompilerParams(
            collective_id=0, has_side_effects=True, vmem_limit_bytes=64000000
        ),
    )(*args)
    return pl.pallas_call(
        store_results,
        name="store_results",
        out_shape=tuple(jax.ShapeDtypeStruct(r.shape, r.dtype) for r in (hidden, state)),
        in_specs=[vmem_spec] * 2,
        out_specs=(hbm_spec, hbm_spec),
        scratch_shapes=[dma((2,))],
    )(*[pltpu.with_memory_space_constraint(r, pltpu.VMEM) for r in results])


def solution(mesh):
    return jax.shard_map(
        functools.partial(per_device, mesh.shape["tp"], mesh.shape["dp"]),
        mesh=mesh,
        in_specs=(
            P(("grp", "tp"), "dp"),
            P(None, "dp"),
            P(None, "dp", "tp"),
            P(None, "dp", "tp"),
            P(None, "dp", "tp"),
            P(None, "dp", "tp"),
            P(None, "dp", "tp"),
            P(None, "tp"),
            P(None, "tp", "dp"),
            P(None, ("grp", "dp"), "tp"),
            P(None, ("grp", "dp"), "tp", None, None),
        ),
        out_specs=(P(("grp", "tp"), "dp"), P(None, ("grp", "dp"), "tp", None, None)),
        check_vma=False,
    )
```

```python
import functools

import jax
import jax.numpy as jnp
from jax import lax
from jax.experimental import pallas as pl
from jax.experimental.pallas import tpu as pltpu
from jax.sharding import PartitionSpec as P

D = 4096
HEAD_KEY = 64
VALUE_CHANNELS = 128
LAYERS = 2

epsilon = 1e-06
softness_factor = 16.0

MESH = pl.DeviceIdType.MESH

STEPS = (
    (
        "F1", "A0", "F2", "A1", "F3", "U0", "A2", "F4",
        "U1", "A3", "O0", "U2", "O1", "A4", "U3", "O2",
        "U4", "O3", "O4",
    ),
    (
        "F1", "A0", "F2", "A1", "F3", "U0", "A2", "F4",
        "U1", "A3", "O0", "U2", "A4", "O1", "U3", "U4",
        "O2", "O3", "O4",
    ),
)


def kernel(
    n_tp,
    n_dp,
    hidden,
    gain,
    w_query,
    w_key,
    w_decay,
    w_value,
    w_gate,
    out_gain,
    w_out,
    decay_offset,
    state,
    hidden_out,
    new_state,
    h_v,
    gain_v,
    wqkd,
    wvg,
    ogain_v,
    wout_v,
    off_v,
    st,
    ag,
    part_send,
    part_recv,
    gat,
    terms,
    terms_in,
    xs,
    pk,
    local_sem,
    state_sem,
    ready,
    all_send_sem,
    far_send_sem,
    far_sem,
    mate_send_sem,
    mate_sem,
    part_send_sem,
    part_sem,
    gat_send_sem,
    gat_sem,
    terms_send_sem,
    terms_sem,
):
    rows, feats = h_v.shape
    half = feats // 2
    members = n_tp // n_dp
    seqs = rows * members
    p = lax.axis_index("tp")
    d = lax.axis_index("dp")
    group = p // members
    place = p % members
    anti = (p + n_tp // 2) % n_tp
    last = n_dp - 1

    def mate(j):
        return group * members + (place + 1 + j) % members

    def up(k):
        return (p + members * k) % n_tp

    def down(k):
        return (p - members * k + n_tp) % n_tp

    quads = [up(k) for k in range(1, n_dp // 2 + 1)] + [down(k) for k in range(1, n_dp // 2)]
    barrier = pltpu.get_barrier_semaphore()

    def greet(device):
        pl.semaphore_signal(barrier, inc=1, device_id=device, device_id_type=MESH)

    for j in range(members - 1):
        greet({"tp": mate(j)})
    for peer in quads:

        @pl.when((peer > p) | (peer == p - members))
        def _():
            greet({"tp": peer})

    for j in range(n_dp - 1):
        greet({"dp": (d + 1 + j) % n_dp})
    heard = members - 1 + n_dp - 1
    for peer in quads:
        heard += jnp.where((peer < p) | (peer == p + members), 1, 0)

    fetches = [
        pltpu.make_async_copy(hidden, h_v, local_sem.at[0]),
        pltpu.make_async_copy(gain, gain_v, local_sem.at[1]),
        pltpu.make_async_copy(w_query, wqkd.at[:, pl.ds(0, HEAD_KEY)], local_sem.at[2]),
        pltpu.make_async_copy(w_key, wqkd.at[:, pl.ds(HEAD_KEY, HEAD_KEY)], local_sem.at[3]),
        pltpu.make_async_copy(w_decay, wqkd.at[:, pl.ds(2 * HEAD_KEY, HEAD_KEY)], local_sem.at[4]),
        pltpu.make_async_copy(w_value, wvg.at[:, :, pl.ds(0, 128)], local_sem.at[5]),
        pltpu.make_async_copy(w_gate, wvg.at[:, :, pl.ds(128, 128)], local_sem.at[6]),
        pltpu.make_async_copy(out_gain, ogain_v, local_sem.at[7]),
        pltpu.make_async_copy(w_out, wout_v, local_sem.at[8]),
        pltpu.make_async_copy(decay_offset, off_v, local_sem.at[9]),
    ]
    for f in fetches:
        f.start()
    state_in = [
        pltpu.make_async_copy(state.at[l, :, 0], st.at[l], state_sem.at[l]) for l in range(LAYERS)
    ]
    for f in state_in:
        f.start()

    xs[...] = jnp.zeros_like(xs)
    wqkd[:, 3 * HEAD_KEY :, :] = jnp.zeros_like(wqkd[:, 3 * HEAD_KEY :, :])

    fetches[0].wait()
    first = h_v[...].astype(jnp.float32)
    pk[0, 0:1, 0:feats] = first[0:1]
    pk[0, 0:1, feats : feats + half] = first[1:2, 0:half]
    pk[0, 1:2, 0:half] = first[1:2, half:feats]
    pk[0, 1:2, half : half + feats] = first[2:3]
    ag[0, p] = pk[0].astype(jnp.bfloat16)

    with jax.named_scope("barrier"):
        pl.semaphore_wait(barrier, heard)

    @pl.when(up(1) < p)
    def _():
        pl.semaphore_signal(ready, inc=1, device_id={"tp": up(1)}, device_id_type=MESH)

    def offset(i):
        k = (i + 1) // 2
        return jnp.where(i % 2 == 1, n_dp - k, k)

    def source_group(i):
        return (group + offset(i)) % n_dp

    def row_group(l, i):
        return (source_group(i) + l * (n_dp // 2)) % n_dp

    def source(i):
        return source_group(i) * members + place

    def remote(src, dst, send_sem, recv_sem, device):
        return pltpu.make_async_remote_copy(
            src_ref=src,
            dst_ref=dst,
            send_sem=send_sem,
            recv_sem=recv_sem,
            device_id=device,
            device_id_type=MESH,
        )

    def arrived(ref, sem):
        remote(ref, ref, all_send_sem, sem, {"tp": anti}).wait_recv()

    def far_copy(sigma, i, to, relayed):
        return remote(
            ag.at[0, sigma], ag.at[0, sigma], far_send_sem.at[relayed, i], far_sem.at[0, i], {"tp": to}
        )

    def own_rows(act):
        for k in range(n_dp // 2, 0, -1):
            for i, to in ((2 * k - 1, up(k)), (2 * k, down(k))):
                if i == n_dp:
                    continue

                @pl.when((to < p) | (to == p + members))
                def _():
                    act(far_copy(p, i, to, 0))

    def across(act):
        @pl.when(down(1) > p)
        def _():
            act(far_copy(p, 2, down(1), 0))

    def relay(i, act):
        sigma = source(i)
        to = up(1) if i % 2 == 1 else down(1)

        @pl.when(to > sigma)
        def _():
            act(far_copy(sigma, i + 2, to, 1))

    def to_mates(l, i):
        sigma = source(i)
        for j in range(members - 1):
            remote(
                ag.at[l, sigma],
                ag.at[l, sigma],
                mate_send_sem.at[l],
                mate_sem.at[l, i],
                {"tp": mate(j)},
            ).start()

    def begin(l):
        if l == 0:
            own_rows(lambda copy: copy.start())
            to_mates(l, 0)

            @pl.when(down(1) > p)
            def _():
                pl.semaphore_wait(ready, 1)

            across(lambda copy: copy.start())
        else:
            for k in range(n_dp // 2, 0, -1):
                for i, to in ((2 * k - 1, up(k)), (2 * k, down(k))):
                    if i < n_dp:
                        remote(
                            ag.at[l, p], ag.at[l, p], all_send_sem, far_sem.at[l, i], {"tp": to}
                        ).start()
            to_mates(l, 0)

    def forward(l, i):
        arrived(ag.at[l, source(i)], far_sem.at[l, i])
        if l == 0 and i + 2 < n_dp:
            relay(i, lambda copy: copy.start())
        to_mates(l, i)

    lane = lax.broadcasted_iota(jnp.int32, (seqs, 512), 1)

    def project(l, i):
        sg = source_group(i)
        arrived(ag.at[l, pl.ds(0, members - 1)], mate_sem.at[l, i])
        for j in range(members):
            b = ag[l, sg * members + j].astype(jnp.float32)
            xs[3 * j : 3 * j + 1, :] = b[0:1, 0:feats]
            xs[3 * j + 1 : 3 * j + 2, 0:half] = b[0:1, feats : feats + half]
            xs[3 * j + 1 : 3 * j + 2, half:feats] = b[1:2, 0:half]
            xs[3 * j + 2 : 3 * j + 3, :] = b[1:2, half : half + feats]
        x = xs[...]
        squares = jnp.sum(x * x, axis=1, keepdims=True)[0:seqs]
        scaled = (x * gain_v[l : l + 1, :]).astype(jnp.bfloat16)
        y = jnp.concatenate(
            [
                lax.dot_general(
                    scaled,
                    wqkd[l],
                    (((1,), (1,)), ((), ())),
                    preferred_element_type=jnp.float32,
                ),
                jnp.dot(scaled, wvg[l], preferred_element_type=jnp.float32),
            ],
            axis=1,
        )[0:seqs]
        high = squares.astype(jnp.bfloat16).astype(jnp.float32)
        rest = squares - high
        mid = rest.astype(jnp.bfloat16).astype(jnp.float32)
        low = rest - mid
        y = jnp.where(lane == 192, high, y)
        y = jnp.where(lane == 193, mid, y)
        y = jnp.where(lane == 194, low, y)
        part_send[l, i] = y.astype(jnp.bfloat16)
        to = row_group(l, i)

        @pl.when(to != d)
        def _():
            slot = (d - to + n_dp) % n_dp - 1
            remote(
                part_send.at[l, i],
                part_recv.at[l, slot],
                part_send_sem.at[l],
                part_sem.at[l],
                {"dp": to},
            ).start()

    def gat_copy(l, i, peer):
        return remote(
            gat.at[l, i], gat.at[l, i], gat_send_sem.at[l], gat_sem.at[l, i], {"dp": peer}
        )

    def update(l, i):
        arrived(part_recv.at[l], part_sem.at[l])
        total = part_send[l, i].astype(jnp.float32)
        for k in range(n_dp - 1):
            total += part_recv[l, k].astype(jnp.float32)
        squares = jnp.sum(total[:, 192:195], axis=1, keepdims=True)
        projected = total * lax.rsqrt(squares / D + epsilon)
        query_key = projected[:, 0:128]
        decay_pre = projected[:, 128:256]
        value = projected[:, 256:384]
        gate = projected[:, 384:512]
        log_sig = jnp.minimum(decay_pre, 0.0) - jnp.log1p(jnp.exp(-jnp.abs(decay_pre)))
        rate = jnp.exp(log_sig[:, 0:HEAD_KEY] / softness_factor + off_v[:, l, :])
        query = query_key[:, 0:HEAD_KEY]
        key = query_key[:, HEAD_KEY : 2 * HEAD_KEY] * HEAD_KEY ** (-0.5)
        columns = jnp.transpose(jnp.concatenate([query * rate, rate], axis=1), (1, 0))
        outs = []
        for s in range(seqs):
            weight = columns[0:HEAD_KEY, s : s + 1]
            outs.append(jnp.sum(weight * st[l, s], axis=0, keepdims=True))
        readout = jnp.concatenate(outs, axis=0)
        readout += jnp.sum(query * key, axis=1, keepdims=True) * value
        normed = readout * lax.rsqrt(jnp.mean(readout * readout, axis=1, keepdims=True) + epsilon)
        normed = normed * ogain_v[l : l + 1, :]
        silu = gate / (1.0 + jnp.exp(-gate))
        gat[l, i] = (normed * silu).astype(jnp.bfloat16)
        for j in range(n_dp - 1):
            gat_copy(l, i, (d + 1 + j) % n_dp).start()
        columns_key = jnp.transpose(jnp.concatenate([key, key], axis=1), (1, 0))
        for s in range(seqs):
            r = columns[HEAD_KEY : 2 * HEAD_KEY, s : s + 1]
            k = columns_key[0:HEAD_KEY, s : s + 1]
            new_state[l, s, 0] = r * st[l, s] + k * value[s : s + 1, :]

    def out_project(l, i):
        @pl.when(row_group(l, i) != d)
        def _():
            arrived(gat.at[l, i], gat_sem.at[l, i])

        y = jnp.dot(gat[l, i], wout_v[l], preferred_element_type=jnp.float32)
        for j in range(members):
            pk[j, 0:1, 0:feats] = y[3 * j : 3 * j + 1]
            pk[j, 0:1, feats : feats + half] = y[3 * j + 1 : 3 * j + 2, 0:half]
            pk[j, 1:2, 0:half] = y[3 * j + 1 : 3 * j + 2, half:feats]
            pk[j, 1:2, half : half + feats] = y[3 * j + 2 : 3 * j + 3]
        for j in range(members):
            terms[l, members * i + j] = pk[j].astype(jnp.bfloat16)
        base = source_group(i) * members + n_tp // 2
        for j in range(members):
            owner = (base + j) % n_tp

            @pl.when(owner != p)
            def _():
                remote(
                    terms.at[l, members * i + j],
                    terms_in.at[l, (p - owner + n_tp) % n_tp - 1],
                    terms_send_sem.at[l],
                    terms_sem.at[l],
                    {"tp": owner},
                ).start()

    def nearby(k):
        return [i for i in (2 * k - 1, 2 * k) if 0 <= i < n_dp]

    def mine(l, k):
        wanted = [row_group(l, i) == d for i in nearby(k)]

        @pl.when(functools.reduce(jnp.logical_or, wanted))
        def _():
            update(l, jnp.where(wanted[0], nearby(k)[0], nearby(k)[-1]))

    for l in range(LAYERS):
        begin(l)
        if l == 0:
            for f in fetches[1:]:
                f.wait()
        state_in[l].wait()
        for step in STEPS[l]:
            k = int(step[1:])
            if step[0] == "U":
                mine(l, k)
            else:
                fn = {"F": forward, "A": project, "O": out_project}[step[0]]
                order = nearby(k)
                if l > 0 and len(order) == 2:
                    upper = group < n_dp // 2
                    order = [jnp.where(upper, order[1], order[0]), jnp.where(upper, order[0], order[1])]
                for i in order:
                    fn(l, i)

        with jax.named_scope("owner_wait"):
            arrived(terms_in.at[l], terms_sem.at[l])
        total = terms[l, members * last + place].astype(jnp.float32)
        total += jnp.sum(terms_in[l].astype(jnp.float32), axis=0)
        result = (total + ag[l, anti].astype(jnp.float32)).astype(jnp.bfloat16)
        if l + 1 < LAYERS:
            ag[l + 1, p] = result
        else:
            b = result.astype(jnp.float32)
            xs[0:1, :] = b[0:1, 0:feats]
            xs[1:2, 0:half] = b[0:1, feats : feats + half]
            xs[1:2, half:feats] = b[1:2, 0:half]
            xs[2:3, :] = b[1:2, half : half + feats]
            hidden_out[...] = xs[0:rows, :].astype(jnp.bfloat16)

    for l in range(LAYERS):
        for ref, sem in (
            (terms_in.at[l], terms_send_sem),
            (part_recv.at[l], part_send_sem),
            (gat.at[l, pl.ds(0, n_dp - 1)], gat_send_sem),
        ):
            remote(ref, ref, sem.at[l], part_sem.at[l], {"tp": anti}).wait_send()
    for ref, sem in (
        (ag.at[0, pl.ds(0, (members - 1) * n_dp)], mate_send_sem.at[0]),
        (ag.at[1, pl.ds(0, (members - 1) * n_dp)], mate_send_sem.at[1]),
        (ag.at[1, pl.ds(0, n_dp - 1)], all_send_sem),
    ):
        remote(ref, ref, sem, part_sem.at[0], {"tp": anti}).wait_send()
    own_rows(lambda copy: copy.wait_send())
    across(lambda copy: copy.wait_send())
    for i in range(1, n_dp - 2):
        relay(i, lambda copy: copy.wait_send())


def store_results(h, s, h_out, s_out, sem):
    copies = [
        pltpu.make_async_copy(s, s_out, sem.at[0]),
        pltpu.make_async_copy(h, h_out, sem.at[1]),
    ]
    for c in copies:
        c.start()
    for c in copies:
        c.wait()


def per_device(n_tp, n_dp, *args):
    hidden, state = args[0], args[10]
    rows, feats = hidden.shape
    members = n_tp // n_dp
    seqs = state.shape[1]
    block = (2, rows * feats // 2)
    hbm_spec = pl.BlockSpec(memory_space=pltpu.HBM)
    vmem_spec = pl.BlockSpec(memory_space=pltpu.VMEM)
    args = list(args)
    for i in (2, 3, 4):
        args[i] = jnp.swapaxes(args[i], 1, 2)
    args[9] = jnp.swapaxes(args[9], 0, 1)
    bf16, f32 = jnp.bfloat16, jnp.float32
    cols = 512
    dma = pltpu.SemaphoreType.DMA
    results = pl.pallas_call(
        functools.partial(kernel, n_tp, n_dp),
        name="decode",
        out_shape=(
            pltpu.VMEM(hidden.shape, hidden.dtype),
            pltpu.VMEM(state.shape, state.dtype),
        ),
        in_specs=[hbm_spec] * 11,
        out_specs=(vmem_spec, vmem_spec),
        scratch_shapes=[
            pltpu.VMEM(hidden.shape, bf16),
            pltpu.VMEM(args[1].shape, f32),
            pltpu.VMEM((LAYERS, 4 * HEAD_KEY, feats), bf16),
            pltpu.VMEM((LAYERS, feats, 2 * VALUE_CHANNELS), bf16),
            pltpu.VMEM(args[7].shape, f32),
            pltpu.VMEM(args[8].shape, bf16),
            pltpu.VMEM(args[9].shape, f32),
            pltpu.VMEM((LAYERS, seqs) + state.shape[3:], f32),
            pltpu.VMEM((LAYERS, n_tp) + block, bf16),
            pltpu.VMEM((LAYERS, n_dp, seqs, cols), bf16),
            pltpu.VMEM((LAYERS, n_dp - 1, seqs, cols), bf16),
            pltpu.VMEM((LAYERS, n_dp, seqs, VALUE_CHANNELS), bf16),
            pltpu.VMEM((LAYERS, n_tp) + block, bf16),
            pltpu.VMEM((LAYERS, n_tp - 1) + block, bf16),
            pltpu.VMEM((16, feats), f32),
            pltpu.VMEM((members,) + block, f32),
            dma((10,)),
            dma((LAYERS,)),
            pltpu.SemaphoreType.REGULAR,
            dma(()),
            dma((2, n_dp)),
            dma((LAYERS, n_dp)),
            dma((LAYERS,)),
            dma((LAYERS, n_dp)),
            dma((LAYERS,)),
            dma((LAYERS,)),
            dma((LAYERS,)),
            dma((LAYERS, n_dp)),
            dma((LAYERS,)),
            dma((LAYERS,)),
        ],
        compiler_params=pltpu.CompilerParams(
            collective_id=0, has_side_effects=True, vmem_limit_bytes=64000000
        ),
    )(*args)
    return pl.pallas_call(
        store_results,
        name="store_results",
        out_shape=tuple(jax.ShapeDtypeStruct(r.shape, r.dtype) for r in (hidden, state)),
        in_specs=[vmem_spec] * 2,
        out_specs=(hbm_spec, hbm_spec),
        scratch_shapes=[dma((2,))],
    )(*[pltpu.with_memory_space_constraint(r, pltpu.VMEM) for r in results])


def solution(mesh):
    return jax.shard_map(
        functools.partial(per_device, mesh.shape["tp"], mesh.shape["dp"]),
        mesh=mesh,
        in_specs=(
            P(("grp", "tp"), "dp"),
            P(None, "dp"),
            P(None, "dp", "tp"),
            P(None, "dp", "tp"),
            P(None, "dp", "tp"),
            P(None, "dp", "tp"),
            P(None, "dp", "tp"),
            P(None, "tp"),
            P(None, "tp", "dp"),
            P(None, ("grp", "dp"), "tp"),
            P(None, ("grp", "dp"), "tp", None, None),
        ),
        out_specs=(P(("grp", "tp"), "dp"), P(None, ("grp", "dp"), "tp", None, None)),
        check_vma=False,
    )
```

```python
import functools

import jax
import jax.numpy as jnp
from jax import lax
from jax.experimental import pallas as pl
from jax.experimental.pallas import tpu as pltpu
from jax.sharding import PartitionSpec as P

D = 4096
HEAD_KEY = 64
VALUE_CHANNELS = 128
LAYERS = 2

epsilon = 1e-06
softness_factor = 16.0

MESH = pl.DeviceIdType.MESH

STEPS = (
    (
        "F1", "A0", "F2", "A1", "F3", "U0", "A2", "F4",
        "U1", "A3", "O0", "U2", "O1", "A4", "U3", "O2",
        "U4", "O3", "O4",
    ),
    (
        "F1", "A0", "F2", "A1", "F3", "U0", "A2", "F4",
        "U1", "A3", "O0", "U2", "A4", "O1", "U3", "U4",
        "O2", "O3", "O4",
    ),
)


def kernel(
    n_tp,
    n_dp,
    hidden,
    gain,
    w_query,
    w_key,
    w_decay,
    w_value,
    w_gate,
    out_gain,
    w_out,
    decay_offset,
    state,
    hidden_out,
    new_state,
    h_v,
    gain_v,
    wqkd,
    wvg,
    ogain_v,
    wout_v,
    off_v,
    st,
    ag,
    part_send,
    part_recv,
    gat,
    terms,
    terms_in,
    xs,
    pk,
    local_sem,
    state_sem,
    ready,
    all_send_sem,
    far_send_sem,
    far_sem,
    mate_send_sem,
    mate_sem,
    part_send_sem,
    part_sem,
    gat_send_sem,
    gat_sem,
    terms_send_sem,
    terms_sem,
):
    rows, feats = h_v.shape
    half = feats // 2
    members = n_tp // n_dp
    seqs = rows * members
    p = lax.axis_index("tp")
    d = lax.axis_index("dp")
    group = p // members
    place = p % members
    anti = (p + n_tp // 2) % n_tp
    last = n_dp - 1

    def mate(j):
        return group * members + (place + 1 + j) % members

    def up(k):
        return (p + members * k) % n_tp

    def down(k):
        return (p - members * k + n_tp) % n_tp

    quads = [up(k) for k in range(1, n_dp // 2 + 1)] + [down(k) for k in range(1, n_dp // 2)]
    barrier = pltpu.get_barrier_semaphore()

    def greet(device):
        pl.semaphore_signal(barrier, inc=1, device_id=device, device_id_type=MESH)

    for j in range(members - 1):
        greet({"tp": mate(j)})
    for peer in quads:

        @pl.when((peer > p) | (peer == p - members))
        def _():
            greet({"tp": peer})

    for j in range(n_dp - 1):
        greet({"dp": (d + 1 + j) % n_dp})
    heard = members - 1 + n_dp - 1
    for peer in quads:
        heard += jnp.where((peer < p) | (peer == p + members), 1, 0)

    fetches = [
        pltpu.make_async_copy(hidden, h_v, local_sem.at[0]),
        pltpu.make_async_copy(gain, gain_v, local_sem.at[1]),
        pltpu.make_async_copy(w_query, wqkd.at[:, pl.ds(0, HEAD_KEY)], local_sem.at[2]),
        pltpu.make_async_copy(w_key, wqkd.at[:, pl.ds(HEAD_KEY, HEAD_KEY)], local_sem.at[3]),
        pltpu.make_async_copy(w_decay, wqkd.at[:, pl.ds(2 * HEAD_KEY, HEAD_KEY)], local_sem.at[4]),
        pltpu.make_async_copy(w_value, wvg.at[:, :, pl.ds(0, 128)], local_sem.at[5]),
        pltpu.make_async_copy(w_gate, wvg.at[:, :, pl.ds(128, 128)], local_sem.at[6]),
        pltpu.make_async_copy(out_gain, ogain_v, local_sem.at[7]),
        pltpu.make_async_copy(w_out, wout_v, local_sem.at[8]),
        pltpu.make_async_copy(decay_offset, off_v, local_sem.at[9]),
    ]
    for f in fetches:
        f.start()
    state_in = [
        pltpu.make_async_copy(state.at[l, :, 0], st.at[l], state_sem.at[l]) for l in range(LAYERS)
    ]
    for f in state_in:
        f.start()

    xs[...] = jnp.zeros_like(xs)
    wqkd[:, 3 * HEAD_KEY :, :] = jnp.zeros_like(wqkd[:, 3 * HEAD_KEY :, :])

    fetches[0].wait()
    first = h_v[...].astype(jnp.float32)
    pk[0, 0:1, 0:feats] = first[0:1]
    pk[0, 0:1, feats : feats + half] = first[1:2, 0:half]
    pk[0, 1:2, 0:half] = first[1:2, half:feats]
    pk[0, 1:2, half : half + feats] = first[2:3]
    ag[0, p] = pk[0].astype(jnp.bfloat16)

    with jax.named_scope("barrier"):
        pl.semaphore_wait(barrier, heard)

    @pl.when(up(1) < p)
    def _():
        pl.semaphore_signal(ready, inc=1, device_id={"tp": up(1)}, device_id_type=MESH)

    def offset(i):
        k = (i + 1) // 2
        return jnp.where(i % 2 == 1, n_dp - k, k)

    def source_group(i):
        return (group + offset(i)) % n_dp

    def row_group(l, i):
        return (source_group(i) + l * (n_dp // 2)) % n_dp

    def source(i):
        return source_group(i) * members + place

    def remote(src, dst, send_sem, recv_sem, device):
        return pltpu.make_async_remote_copy(
            src_ref=src,
            dst_ref=dst,
            send_sem=send_sem,
            recv_sem=recv_sem,
            device_id=device,
            device_id_type=MESH,
        )

    def arrived(ref, sem):
        remote(ref, ref, all_send_sem, sem, {"tp": anti}).wait_recv()

    def far_copy(sigma, i, to, relayed):
        return remote(
            ag.at[0, sigma], ag.at[0, sigma], far_send_sem.at[relayed, i], far_sem.at[0, i], {"tp": to}
        )

    def own_rows(act):
        for k in range(n_dp // 2, 0, -1):
            for i, to in ((2 * k - 1, up(k)), (2 * k, down(k))):
                if i == n_dp:
                    continue

                @pl.when((to < p) | (to == p + members))
                def _():
                    act(far_copy(p, i, to, 0))

    def across(act):
        @pl.when(down(1) > p)
        def _():
            act(far_copy(p, 2, down(1), 0))

    def relay(i, act):
        sigma = source(i)
        to = up(1) if i % 2 == 1 else down(1)

        @pl.when(to > sigma)
        def _():
            act(far_copy(sigma, i + 2, to, 1))

    def to_mates(l, i):
        sigma = source(i)
        for j in range(members - 1):
            remote(
                ag.at[l, sigma],
                ag.at[l, sigma],
                mate_send_sem.at[l],
                mate_sem.at[l, i],
                {"tp": mate(j)},
            ).start()

    def begin(l):
        if l == 0:
            own_rows(lambda copy: copy.start())
            to_mates(l, 0)

            @pl.when(down(1) > p)
            def _():
                pl.semaphore_wait(ready, 1)

            across(lambda copy: copy.start())
        else:
            for k in range(n_dp // 2, 0, -1):
                for i, to in ((2 * k - 1, up(k)), (2 * k, down(k))):
                    if i < n_dp:
                        remote(
                            ag.at[l, p], ag.at[l, p], all_send_sem, far_sem.at[l, i], {"tp": to}
                        ).start()
            to_mates(l, 0)

    def forward(l, i):
        arrived(ag.at[l, source(i)], far_sem.at[l, i])
        if l == 0 and i + 2 < n_dp:
            relay(i, lambda copy: copy.start())
        to_mates(l, i)

    lane = lax.broadcasted_iota(jnp.int32, (seqs, 512), 1)

    def project(l, i):
        sg = source_group(i)
        arrived(ag.at[l, pl.ds(0, members - 1)], mate_sem.at[l, i])
        for j in range(members):
            b = ag[l, sg * members + j].astype(jnp.float32)
            xs[3 * j : 3 * j + 1, :] = b[0:1, 0:feats]
            xs[3 * j + 1 : 3 * j + 2, 0:half] = b[0:1, feats : feats + half]
            xs[3 * j + 1 : 3 * j + 2, half:feats] = b[1:2, 0:half]
            xs[3 * j + 2 : 3 * j + 3, :] = b[1:2, half : half + feats]
        x = xs[...]
        squares = jnp.sum(x * x, axis=1, keepdims=True)[0:seqs]
        scaled = (x * gain_v[l : l + 1, :]).astype(jnp.bfloat16)
        y = jnp.concatenate(
            [
                lax.dot_general(
                    scaled,
                    wqkd[l],
                    (((1,), (1,)), ((), ())),
                    preferred_element_type=jnp.float32,
                ),
                jnp.dot(scaled, wvg[l], preferred_element_type=jnp.float32),
            ],
            axis=1,
        )[0:seqs]
        high = squares.astype(jnp.bfloat16).astype(jnp.float32)
        rest = squares - high
        mid = rest.astype(jnp.bfloat16).astype(jnp.float32)
        low = rest - mid
        y = jnp.where(lane == 192, high, y)
        y = jnp.where(lane == 193, mid, y)
        y = jnp.where(lane == 194, low, y)
        part_send[l, i] = y.astype(jnp.bfloat16)
        to = row_group(l, i)

        @pl.when(to != d)
        def _():
            slot = (d - to + n_dp) % n_dp - 1
            remote(
                part_send.at[l, i],
                part_recv.at[l, slot],
                part_send_sem.at[l],
                part_sem.at[l],
                {"dp": to},
            ).start()

    def gat_copy(l, i, peer):
        return remote(
            gat.at[l, i], gat.at[l, i], gat_send_sem.at[l], gat_sem.at[l, i], {"dp": peer}
        )

    def update(l, i):
        arrived(part_recv.at[l], part_sem.at[l])
        total = part_send[l, i].astype(jnp.float32)
        for k in range(n_dp - 1):
            total += part_recv[l, k].astype(jnp.float32)
        squares = jnp.sum(total[:, 192:195], axis=1, keepdims=True)
        projected = total * lax.rsqrt(squares / D + epsilon)
        query_key = projected[:, 0:128]
        decay_pre = projected[:, 128:256]
        value = projected[:, 256:384]
        gate = projected[:, 384:512]
        log_sig = jnp.minimum(decay_pre, 0.0) - jnp.log1p(jnp.exp(-jnp.abs(decay_pre)))
        rate = jnp.exp(log_sig[:, 0:HEAD_KEY] / softness_factor + off_v[:, l, :])
        query = query_key[:, 0:HEAD_KEY]
        key = query_key[:, HEAD_KEY : 2 * HEAD_KEY] * HEAD_KEY ** (-0.5)
        columns = jnp.transpose(jnp.concatenate([query * rate, rate], axis=1), (1, 0))
        outs = []
        for s in range(seqs):
            weight = columns[0:HEAD_KEY, s : s + 1]
            outs.append(jnp.sum(weight * st[l, s], axis=0, keepdims=True))
        readout = jnp.concatenate(outs, axis=0)
        readout += jnp.sum(query * key, axis=1, keepdims=True) * value
        normed = readout * lax.rsqrt(jnp.mean(readout * readout, axis=1, keepdims=True) + epsilon)
        normed = normed * ogain_v[l : l + 1, :]
        silu = gate / (1.0 + jnp.exp(-gate))
        gat[l, i] = (normed * silu).astype(jnp.bfloat16)
        for j in range(n_dp - 1):
            gat_copy(l, i, (d + 1 + j) % n_dp).start()
        columns_key = jnp.transpose(jnp.concatenate([key, key], axis=1), (1, 0))
        for s in range(seqs):
            r = columns[HEAD_KEY : 2 * HEAD_KEY, s : s + 1]
            k = columns_key[0:HEAD_KEY, s : s + 1]
            new_state[l, s, 0] = r * st[l, s] + k * value[s : s + 1, :]

    def out_project(l, i):
        @pl.when(row_group(l, i) != d)
        def _():
            arrived(gat.at[l, i], gat_sem.at[l, i])

        y = jnp.dot(gat[l, i], wout_v[l], preferred_element_type=jnp.float32)
        for j in range(members):
            pk[j, 0:1, 0:feats] = y[3 * j : 3 * j + 1]
            pk[j, 0:1, feats : feats + half] = y[3 * j + 1 : 3 * j + 2, 0:half]
            pk[j, 1:2, 0:half] = y[3 * j + 1 : 3 * j + 2, half:feats]
            pk[j, 1:2, half : half + feats] = y[3 * j + 2 : 3 * j + 3]
        for j in range(members):
            terms[l, members * i + j] = pk[j].astype(jnp.bfloat16)
        base = source_group(i) * members + n_tp // 2
        for j in range(members):
            owner = (base + j) % n_tp

            @pl.when(owner != p)
            def _():
                remote(
                    terms.at[l, members * i + j],
                    terms_in.at[l, (p - owner + n_tp) % n_tp - 1],
                    terms_send_sem.at[l],
                    terms_sem.at[l],
                    {"tp": owner},
                ).start()

    def nearby(k):
        return [i for i in (2 * k - 1, 2 * k) if 0 <= i < n_dp]

    def mine(l, k):
        wanted = [row_group(l, i) == d for i in nearby(k)]

        @pl.when(functools.reduce(jnp.logical_or, wanted))
        def _():
            update(l, jnp.where(wanted[0], nearby(k)[0], nearby(k)[-1]))

    for l in range(LAYERS):
        begin(l)
        if l == 0:
            for f in fetches[1:]:
                f.wait()
        state_in[l].wait()
        for step in STEPS[l]:
            k = int(step[1:])
            if step[0] == "U":
                mine(l, k)
            else:
                fn = {"F": forward, "A": project, "O": out_project}[step[0]]
                order = nearby(k)
                if len(order) == 2 and (l > 0 or step[0] != "F"):
                    upper = group < n_dp // 2 if l > 0 else group >= n_dp // 2
                    order = [jnp.where(upper, order[1], order[0]), jnp.where(upper, order[0], order[1])]
                for i in order:
                    fn(l, i)

        with jax.named_scope("owner_wait"):
            arrived(terms_in.at[l], terms_sem.at[l])
        total = terms[l, members * last + place].astype(jnp.float32)
        total += jnp.sum(terms_in[l].astype(jnp.float32), axis=0)
        result = (total + ag[l, anti].astype(jnp.float32)).astype(jnp.bfloat16)
        if l + 1 < LAYERS:
            ag[l + 1, p] = result
        else:
            b = result.astype(jnp.float32)
            xs[0:1, :] = b[0:1, 0:feats]
            xs[1:2, 0:half] = b[0:1, feats : feats + half]
            xs[1:2, half:feats] = b[1:2, 0:half]
            xs[2:3, :] = b[1:2, half : half + feats]
            hidden_out[...] = xs[0:rows, :].astype(jnp.bfloat16)

    for l in range(LAYERS):
        for ref, sem in (
            (terms_in.at[l], terms_send_sem),
            (part_recv.at[l], part_send_sem),
            (gat.at[l, pl.ds(0, n_dp - 1)], gat_send_sem),
        ):
            remote(ref, ref, sem.at[l], part_sem.at[l], {"tp": anti}).wait_send()
    for ref, sem in (
        (ag.at[0, pl.ds(0, (members - 1) * n_dp)], mate_send_sem.at[0]),
        (ag.at[1, pl.ds(0, (members - 1) * n_dp)], mate_send_sem.at[1]),
        (ag.at[1, pl.ds(0, n_dp - 1)], all_send_sem),
    ):
        remote(ref, ref, sem, part_sem.at[0], {"tp": anti}).wait_send()
    own_rows(lambda copy: copy.wait_send())
    across(lambda copy: copy.wait_send())
    for i in range(1, n_dp - 2):
        relay(i, lambda copy: copy.wait_send())


def store_results(h, s, h_out, s_out, sem):
    copies = [
        pltpu.make_async_copy(s, s_out, sem.at[0]),
        pltpu.make_async_copy(h, h_out, sem.at[1]),
    ]
    for c in copies:
        c.start()
    for c in copies:
        c.wait()


def per_device(n_tp, n_dp, *args):
    hidden, state = args[0], args[10]
    rows, feats = hidden.shape
    members = n_tp // n_dp
    seqs = state.shape[1]
    block = (2, rows * feats // 2)
    hbm_spec = pl.BlockSpec(memory_space=pltpu.HBM)
    vmem_spec = pl.BlockSpec(memory_space=pltpu.VMEM)
    args = list(args)
    for i in (2, 3, 4):
        args[i] = jnp.swapaxes(args[i], 1, 2)
    args[9] = jnp.swapaxes(args[9], 0, 1)
    bf16, f32 = jnp.bfloat16, jnp.float32
    cols = 512
    dma = pltpu.SemaphoreType.DMA
    results = pl.pallas_call(
        functools.partial(kernel, n_tp, n_dp),
        name="decode",
        out_shape=(
            pltpu.VMEM(hidden.shape, hidden.dtype),
            pltpu.VMEM(state.shape, state.dtype),
        ),
        in_specs=[hbm_spec] * 11,
        out_specs=(vmem_spec, vmem_spec),
        scratch_shapes=[
            pltpu.VMEM(hidden.shape, bf16),
            pltpu.VMEM(args[1].shape, f32),
            pltpu.VMEM((LAYERS, 4 * HEAD_KEY, feats), bf16),
            pltpu.VMEM((LAYERS, feats, 2 * VALUE_CHANNELS), bf16),
            pltpu.VMEM(args[7].shape, f32),
            pltpu.VMEM(args[8].shape, bf16),
            pltpu.VMEM(args[9].shape, f32),
            pltpu.VMEM((LAYERS, seqs) + state.shape[3:], f32),
            pltpu.VMEM((LAYERS, n_tp) + block, bf16),
            pltpu.VMEM((LAYERS, n_dp, seqs, cols), bf16),
            pltpu.VMEM((LAYERS, n_dp - 1, seqs, cols), bf16),
            pltpu.VMEM((LAYERS, n_dp, seqs, VALUE_CHANNELS), bf16),
            pltpu.VMEM((LAYERS, n_tp) + block, bf16),
            pltpu.VMEM((LAYERS, n_tp - 1) + block, bf16),
            pltpu.VMEM((16, feats), f32),
            pltpu.VMEM((members,) + block, f32),
            dma((10,)),
            dma((LAYERS,)),
            pltpu.SemaphoreType.REGULAR,
            dma(()),
            dma((2, n_dp)),
            dma((LAYERS, n_dp)),
            dma((LAYERS,)),
            dma((LAYERS, n_dp)),
            dma((LAYERS,)),
            dma((LAYERS,)),
            dma((LAYERS,)),
            dma((LAYERS, n_dp)),
            dma((LAYERS,)),
            dma((LAYERS,)),
        ],
        compiler_params=pltpu.CompilerParams(
            collective_id=0, has_side_effects=True, vmem_limit_bytes=64000000
        ),
    )(*args)
    return pl.pallas_call(
        store_results,
        name="store_results",
        out_shape=tuple(jax.ShapeDtypeStruct(r.shape, r.dtype) for r in (hidden, state)),
        in_specs=[vmem_spec] * 2,
        out_specs=(hbm_spec, hbm_spec),
        scratch_shapes=[dma((2,))],
    )(*[pltpu.with_memory_space_constraint(r, pltpu.VMEM) for r in results])


def solution(mesh):
    return jax.shard_map(
        functools.partial(per_device, mesh.shape["tp"], mesh.shape["dp"]),
        mesh=mesh,
        in_specs=(
            P(("grp", "tp"), "dp"),
            P(None, "dp"),
            P(None, "dp", "tp"),
            P(None, "dp", "tp"),
            P(None, "dp", "tp"),
            P(None, "dp", "tp"),
            P(None, "dp", "tp"),
            P(None, "tp"),
            P(None, "tp", "dp"),
            P(None, ("grp", "dp"), "tp"),
            P(None, ("grp", "dp"), "tp", None, None),
        ),
        out_specs=(P(("grp", "tp"), "dp"), P(None, ("grp", "dp"), "tp", None, None)),
        check_vma=False,
    )
```
